512 devices in a mesh: dp: 4 (over x), kv: 64 (over z, y), tp: 2 (over core).
Axes of the slice: x: 4, y: 8, z: 8, core: 2. Of those that a mesh axis runs over, the one named last changes fastest.
Arguments:
- hidden: bfloat16 [2048, 256], P(('kv', 'tp'), 'dp'), parts along dimension 1, may hold values from -20 to 20
- mixer_gain: float32 [2048], replicated, may hold values from 0.1 to 1.9
- gate_proj: bfloat16 [2048, 64, 64], P(None, 'kv', 'tp'), may hold values from -0.125 to 0.125
- inner_proj: bfloat16 [2048, 64, 64], P(None, 'kv', 'tp'), may hold values from -0.125 to 0.125
- input_proj: bfloat16 [2048, 1024], P(None, 'kv'), may hold values from -0.125 to 0.125
- output_proj: bfloat16 [2048, 1024], P(None, 'kv'), may hold values from -0.125 to 0.125
- step_proj: bfloat16 [2048, 64], replicated, may hold values from -0.125 to 0.125
- step_bias: float32 [64], replicated, may hold values from -3 to -0.5
- decay_log: float32 [64], replicated, may hold values from -3 to 1
- skip_gain: float32 [64], replicated, may hold values from 0.3 to 1.5
- taps_inner: float32 [4, 64, 64], P(None, None, 'tp'), may hold values from -3 to 3
- taps_input: float32 [4, 1024], replicated, may hold values from -3 to 3
- taps_output: float32 [4, 1024], replicated, may hold values from -3 to 3
- recent_inner: bfloat16 [256, 3, 64, 64], P(('dp', 'kv'), None, None, 'tp'), parts along dimension 0, may hold values from -6 to 6
- recent_input: bfloat16 [256, 3, 1024], P(('dp', 'kv')), parts along dimension 0, may hold values from -6 to 6
- recent_output: bfloat16 [256, 3, 1024], P(('dp', 'kv')), parts along dimension 0, may hold values from -6 to 6
- states: float32 [256, 64, 64, 128], P(('dp', 'kv'), None, 'tp'), parts along dimension 0, may hold values from -4 to 4
- block_inner: bfloat16 [256, 128, 64, 64], P(('dp', 'kv'), None, None, 'tp'), parts along dimension 0, may hold values from -6 to 6
- block_input: bfloat16 [256, 128, 1024], P(('dp', 'kv')), parts along dimension 0, may hold values from -4 to 4
- block_decay: float32 [256, 128, 64], P(('dp', 'kv')), parts along dimension 0
- lengths: int32 [256], P(('dp', 'kv')), parts along dimension 0, may hold values from 1 to 128, 2730 in all
- norm_gain: float32 [64, 64], P(None, 'tp'), may hold values from 0.1 to 1.9
- mixer_out: bfloat16 [64, 64, 2048], P('kv', 'tp'), may hold values from -0.25 to 0.25
- channel_gain: float32 [2048], replicated, may hold values from 0.1 to 1.9
- expand_gate: bfloat16 [2048, 5632], P(None, ('kv', 'tp')), may hold values from -0.125 to 0.125
- expand_value: bfloat16 [2048, 5632], P(None, ('kv', 'tp')), may hold values from -0.125 to 0.125
- reduce_proj: bfloat16 [5632, 2048], P(('kv', 'tp')), may hold values from -0.3125 to 0.3125
Outputs:
- layer_out: bfloat16 [2048, 256], P(('kv', 'tp'), 'dp'), parts along dimension 1
The draws below stay inside these ranges and needn't reach their ends.
There are 4 independent parts, one for each index of `dp`. The reference program is written for one: setup_inputs(seed, part) draws one part's arguments, and reference() takes and returns one part's arrays. A program takes and returns all parts, laid end to end along the dimension named above; an argument that names none is the same for every part. Nothing has to cross between parts.
All inputs are finite; a program needn't handle non-finite values. No bound on the sum of `lengths` on one device may be relied on, other than what follows from the above.
Results may differ from the reference program's by a relative error of at most 0.01.
Values may be sent and summed in bfloat16 or wider, within the bound.
A program may use at most 64 MiB of HBM per device.

```python
import math
import jax
import jax.numpy as jnp
import numpy as np
from jax import lax

D = 2048
MIXER_HEADS = 64
HEAD_DIM = 64
GROUPS = 8
STATE = 128
FF = 5632
TAPS = 4
OPEN_BLOCK_SPAN = 128
GROUP_SEQUENCES = 64


def draw_hidden(key, part):
    rows = jnp.arange(D, dtype=jnp.float32)[:, None] / D
    rising = 1.0 + 2.0 * rows
    base = jax.random.truncated_normal(key, -4.0, 4.0, (D, GROUP_SEQUENCES), jnp.float32)
    return (base * rising).astype(jnp.bfloat16)


def draw_block_decay(key, part):
    key_rate, key_seq, key_jitter, position_key, extent_key = jax.random.split(jax.random.fold_in(key, 17), 5)
    low, high = (math.log(0.2 / OPEN_BLOCK_SPAN), math.log(0.08))
    arrival_rate = jnp.exp(jax.random.uniform(key_rate, (1, 1, MIXER_HEADS), jnp.float32, low, high))
    sequence_share = jnp.exp(jax.random.uniform(key_seq, (GROUP_SEQUENCES, 1, 1), jnp.float32, math.log(0.5), math.log(2.0)))
    random_shift = jnp.exp(jax.random.uniform(key_jitter, (GROUP_SEQUENCES, OPEN_BLOCK_SPAN, MIXER_HEADS), jnp.float32, -0.35, 0.35))
    surge_position = (jax.random.randint(position_key, (GROUP_SEQUENCES, OPEN_BLOCK_SPAN, 1), 0, OPEN_BLOCK_SPAN) < 3).astype(jnp.float32)
    surge_extent = jax.random.uniform(extent_key, (GROUP_SEQUENCES, OPEN_BLOCK_SPAN, MIXER_HEADS), jnp.float32, 0.22, 0.69)
    return -(arrival_rate * sequence_share * random_shift) - surge_position * surge_extent


def raised(result, own_key, source, target, shards_of, factor):
    def block_of(position):
        return (jnp.arange(result.shape[position]) // (result.shape[position] // shards_of)).reshape((-1,) + (1,) * (result.ndim - 1 - position))

    one_side = jax.random.permutation(own_key, shards_of)[block_of(target)]
    other_side = (block_of(target) + shards_of // 2) % shards_of
    return jnp.where((block_of(source) == one_side) | (block_of(source) == other_side), factor * result, result)


def shard_levels(key, extent, shards, least, high):
    loudness = 1.0
    for position, shards_of in shards:
        draws = jax.random.uniform(jax.random.fold_in(jax.random.fold_in(key, 6), position), (shards_of,), jnp.float32, least / len(shards), high / len(shards))
        loudness = loudness * jnp.repeat(jnp.exp(draws), extent[position] // shards_of).reshape((-1,) + (1,) * (len(extent) - 1 - position))
    return loudness


def profile(count, total, reach, skew):
    portions = [(1 << 20) // math.isqrt(standing ** skew) + 1 for standing in range(2, count + 1)]
    rest, counts = total - reach - (count - 1), [1] * (count - 1)
    while rest > 0:
        movable = [i for i in range(count - 1) if counts[i] < reach]
        whole, budget = sum([portions[i] for i in movable]), rest
        for i in movable:
            extra = min(reach - counts[i], max(1, budget * portions[i] // whole), rest)
            counts[i] = counts[i] + extra
            rest = rest - extra
    return np.array([reach] + counts)


def uneven_parts(own_key, number_of, total, most, lean):
    if number_of == 2:
        one = jax.random.randint(own_key, (), max(1, total - most), min(most, total - 1) + 1)
        return jnp.stack([one, total - one])
    sizes = jnp.asarray(profile(number_of, total, most, lean), jnp.int32)
    pairs = (number_of - 1) // 2
    source_of, sink = sizes[1:1 + 2 * pairs:2], sizes[2:2 + 2 * pairs:2]
    room = jnp.minimum(source_of - 1, most - sink)
    moved = jax.random.randint(jax.random.fold_in(own_key, 1), (pairs,), 0, 1 << 20) % (room + 1)
    sizes = sizes.at[1:1 + 2 * pairs:2].set(source_of - moved).at[2:2 + 2 * pairs:2].set(sink + moved)
    return sizes[jax.random.permutation(jax.random.fold_in(own_key, 2), number_of)]


def centred(rng, shape, deviation, bound, cuts=(), kind=jnp.bfloat16):
    entries = deviation * jax.random.normal(rng, shape, jnp.float32)
    if cuts:
        entries = entries * shard_levels(rng, shape, cuts, -0.22, 0.18)
    return jnp.clip(entries, -bound, bound).astype(kind)


def bell_draw_with(stream_key, dims, width, reach, cuts, heavy, kind=jnp.bfloat16):
    array = width * jax.random.normal(stream_key, dims, jnp.float32)
    if cuts:
        array = array * shard_levels(stream_key, dims, cuts, -0.22, 0.18)
    return jnp.clip(raised(array, jax.random.fold_in(stream_key, 3), *heavy), -reach, reach).astype(kind)


def setup_inputs(seed: int = 0, part: int = 0) -> dict:
    seeds = jax.random.split(jax.random.key(seed), 28)
    part_keys = jax.random.split(jax.random.fold_in(seeds[27], part), 28)
    hidden = draw_hidden(jax.random.fold_in(jax.random.fold_in(seeds[27], part), 71), part)
    mixer_gain = jnp.clip(1.0 + 0.18 * jax.random.normal(seeds[1], (D,), jnp.float32), 0.1, 1.9)
    gate_proj = centred(seeds[2], (D, MIXER_HEADS, HEAD_DIM), D ** -0.5, 0.125, ((1, 64), (2, 2)))
    inner_proj = centred(seeds[3], (D, MIXER_HEADS, HEAD_DIM), D ** -0.5, 0.125, ((1, 64), (2, 2)))
    input_proj = centred(seeds[4], (D, GROUPS * STATE), D ** -0.5, 0.125, ((1, 64),))
    output_proj = centred(seeds[5], (D, GROUPS * STATE), D ** -0.5, 0.125, ((1, 64),))
    step_proj = centred(seeds[6], (D, MIXER_HEADS), D ** -0.5, 0.125)
    step_bias = jnp.clip(jax.random.uniform(seeds[7], (MIXER_HEADS,), jnp.float32, -3.0, -0.5), -3.0, -0.5)
    decay_log = jnp.clip(jax.random.uniform(seeds[8], (MIXER_HEADS,), jnp.float32, -3.0, 1.0), -3.0, 1.0)
    skip_gain = jnp.clip(jax.random.uniform(seeds[9], (MIXER_HEADS,), jnp.float32, 0.3, 1.5), 0.3, 1.5)
    taps_inner = centred(seeds[10], (TAPS, MIXER_HEADS, HEAD_DIM), TAPS ** -0.5, 3.0, ((2, 2),), jnp.float32)
    taps_input = centred(seeds[11], (TAPS, GROUPS * STATE), TAPS ** -0.5, 3.0, (), jnp.float32)
    taps_output = centred(seeds[12], (TAPS, GROUPS * STATE), TAPS ** -0.5, 3.0, (), jnp.float32)
    recent_inner = centred(part_keys[13], (GROUP_SEQUENCES, TAPS - 1, MIXER_HEADS, HEAD_DIM), 1.0, 6.0, ((0, 64), (3, 2)))
    recent_input = centred(part_keys[14], (GROUP_SEQUENCES, TAPS - 1, GROUPS * STATE), 1.0, 6.0, ((0, 64),))
    recent_output = centred(part_keys[15], (GROUP_SEQUENCES, TAPS - 1, GROUPS * STATE), 1.0, 6.0, ((0, 64),))
    states = centred(part_keys[16], (GROUP_SEQUENCES, MIXER_HEADS, HEAD_DIM, STATE), 0.3, 4.0, ((0, 64), (2, 2)), jnp.float32)
    block_inner = centred(part_keys[17], (GROUP_SEQUENCES, OPEN_BLOCK_SPAN, MIXER_HEADS, HEAD_DIM), 0.5, 6.0, ((0, 64), (3, 2)))
    block_input = centred(part_keys[18], (GROUP_SEQUENCES, OPEN_BLOCK_SPAN, GROUPS * STATE), 0.25, 4.0, ((0, 64),))
    block_decay = draw_block_decay(jax.random.fold_in(jax.random.fold_in(seeds[27], part), 71), part)
    lengths = uneven_parts(part_keys[20], GROUP_SEQUENCES, GROUP_SEQUENCES * OPEN_BLOCK_SPAN // 3, OPEN_BLOCK_SPAN, 2).astype(jnp.int32)
    norm_gain = jnp.clip(1.0 + 0.18 * jax.random.normal(seeds[21], (MIXER_HEADS, HEAD_DIM), jnp.float32), 0.1, 1.9)
    mixer_out = bell_draw_with(seeds[22], (MIXER_HEADS, HEAD_DIM, D), (MIXER_HEADS * HEAD_DIM) ** -0.5, 0.25, ((0, 64), (1, 2)), (0, 2, 64, 4.0))
    channel_gain = jnp.clip(1.0 + 0.18 * jax.random.normal(seeds[23], (D,), jnp.float32), 0.1, 1.9)
    expand_gate = centred(seeds[24], (D, FF), D ** -0.5, 0.125, ((1, 128),))
    expand_value = centred(seeds[25], (D, FF), D ** -0.5, 0.125, ((1, 128),))
    reduce_proj = bell_draw_with(seeds[26], (FF, D), FF ** -0.5, 0.3125, ((0, 128),), (0, 1, 128, 5.5))
    return {"hidden": hidden, "mixer_gain": mixer_gain, "gate_proj": gate_proj, "inner_proj": inner_proj, "input_proj": input_proj, "output_proj": output_proj, "step_proj": step_proj, "step_bias": step_bias, "decay_log": decay_log, "skip_gain": skip_gain, "taps_inner": taps_inner, "taps_input": taps_input, "taps_output": taps_output, "recent_inner": recent_inner, "recent_input": recent_input, "recent_output": recent_output, "states": states, "block_inner": block_inner, "block_input": block_input, "block_decay": block_decay, "lengths": lengths, "norm_gain": norm_gain, "mixer_out": mixer_out, "channel_gain": channel_gain, "expand_gate": expand_gate, "expand_value": expand_value, "reduce_proj": reduce_proj}


epsilon = 1e-05

def short_conv(recent, newest, taps):
    window = jnp.concatenate([recent.astype(jnp.float32), newest.astype(jnp.float32)[:, None]], axis=1)
    return jax.nn.silu(lax.optimization_barrier(jnp.sum(window * taps[None], axis=1)))

def reference(hidden, mixer_gain, gate_proj, inner_proj, input_proj, output_proj, step_proj, step_bias, decay_log, skip_gain, taps_inner, taps_input, taps_output, recent_inner, recent_input, recent_output, states, block_inner, block_input, block_decay, lengths, norm_gain, mixer_out, channel_gain, expand_gate, expand_value, reduce_proj):
    hidden_f = hidden.astype(jnp.float32)
    rms_in = lax.rsqrt(lax.optimization_barrier(jnp.mean(hidden_f * hidden_f, axis=0)) + epsilon)
    normed_in = (hidden_f * mixer_gain[:, None]).astype(jnp.bfloat16).astype(jnp.float32)
    gate_pre = (rms_in[:, None, None] * jnp.einsum('ds,dhp->shp', normed_in, gate_proj.astype(jnp.float32))).astype(jnp.bfloat16)
    inner_pre = (rms_in[:, None, None] * jnp.einsum('ds,dhp->shp', normed_in, inner_proj.astype(jnp.float32))).astype(jnp.bfloat16)
    input_pre = (rms_in[:, None] * jnp.einsum('ds,dk->sk', normed_in, input_proj.astype(jnp.float32))).astype(jnp.bfloat16)
    output_pre = (rms_in[:, None] * jnp.einsum('ds,dk->sk', normed_in, output_proj.astype(jnp.float32))).astype(jnp.bfloat16)
    step_pre = (rms_in[:, None] * jnp.einsum('ds,dh->sh', normed_in, step_proj.astype(jnp.float32))).astype(jnp.bfloat16)
    conv_inner = short_conv(recent_inner, inner_pre, taps_inner)
    conv_input = short_conv(recent_input, input_pre, taps_input)
    conv_output = short_conv(recent_output, output_pre, taps_output).astype(jnp.bfloat16)
    step = jax.nn.softplus(step_pre.astype(jnp.float32) + step_bias[None, :])
    new_decay = -jnp.exp(decay_log)[None, :] * step
    seq_count = hidden.shape[1]
    per_group = MIXER_HEADS // GROUPS
    live = (jnp.arange(OPEN_BLOCK_SPAN, dtype=jnp.int32)[None, :] < lengths[:, None]).astype(jnp.float32)
    masked = block_decay * live[:, :, None]
    cached = lax.optimization_barrier(jnp.sum(masked, axis=1))
    tail = new_decay[:, None, :] + cached[:, None, :] - jnp.cumsum(masked, axis=1)
    total = new_decay + cached
    readout = conv_output.astype(jnp.float32).reshape(seq_count, GROUPS, STATE)
    score = jnp.einsum('sgn,sjgn->sgj', readout, block_input.astype(jnp.float32).reshape(seq_count, OPEN_BLOCK_SPAN, GROUPS, STATE))
    score_heads = jnp.repeat(score, per_group, axis=1)
    weight = (live[:, None, :] * jnp.exp(jnp.swapaxes(tail, 1, 2)) * score_heads).astype(jnp.bfloat16)
    from_block = jnp.einsum('shj,sjhp->shp', weight.astype(jnp.float32), block_inner.astype(jnp.float32))
    grouped = states.reshape(seq_count, GROUPS, per_group, HEAD_DIM, STATE)
    from_state = jnp.einsum('sgn,sgrpn->sgrp', readout, grouped, precision=lax.Precision.HIGHEST).reshape(seq_count, MIXER_HEADS, HEAD_DIM)
    own_score = jnp.repeat(lax.optimization_barrier(jnp.sum(readout * conv_input.reshape(seq_count, GROUPS, STATE), axis=-1)), per_group, axis=1)
    mix = from_block + jnp.exp(total)[:, :, None] * from_state + (own_score * step)[:, :, None] * conv_inner + skip_gain[None, :, None] * conv_inner
    gated_raw = mix * jax.nn.silu(gate_pre.astype(jnp.float32))
    rms_gate = lax.rsqrt(lax.optimization_barrier(jnp.mean(gated_raw * gated_raw, axis=(1, 2))) + epsilon)
    gated = (gated_raw * norm_gain[None]).astype(jnp.bfloat16)
    mixed = rms_gate[None, :] * jnp.einsum('shp,hpd->ds', gated.astype(jnp.float32), mixer_out.astype(jnp.float32))
    mid = (hidden_f + mixed).astype(jnp.bfloat16).astype(jnp.float32)
    rms_mid = lax.rsqrt(lax.optimization_barrier(jnp.mean(mid * mid, axis=0)) + epsilon)
    normed_mid = (mid * channel_gain[:, None]).astype(jnp.bfloat16).astype(jnp.float32)
    gate_sum = rms_mid[:, None] * jnp.einsum('ds,df->sf', normed_mid, expand_gate.astype(jnp.float32))
    value_sum = rms_mid[:, None] * jnp.einsum('ds,df->sf', normed_mid, expand_value.astype(jnp.float32))
    act = (jax.nn.silu(gate_sum) * value_sum).astype(jnp.bfloat16)
    channel = jnp.einsum('fd,sf->ds', reduce_proj.astype(jnp.float32), act.astype(jnp.float32))
    return (mid + channel).astype(jnp.bfloat16)
```

```python
import jax
import jax.numpy as jnp
from jax import lax
from jax.experimental import pallas as pl
from jax.experimental.pallas import tpu as pltpu
from jax.sharding import PartitionSpec as P

F32 = jnp.float32
BF16 = jnp.bfloat16
MESH = pl.DeviceIdType.MESH
EPS = 1e-05
N = 64
DP_KV = ("dp", "kv")
KV_TP = ("kv", "tp")
NAMES = (
    "hid",
    "mg",
    "gate",
    "inner",
    "inp",
    "outp",
    "stepw",
    "bias",
    "dlog",
    "skip",
    "tinner",
    "tin",
    "tout",
    "rinner",
    "rin",
    "rout",
    "states",
    "binner",
    "binput",
    "bdecay",
    "lens",
    "normg",
    "mo",
    "cg",
    "eg",
    "ev",
    "rp",
)


def silu(v):
    return v / (1.0 + jnp.exp(-v))


def iota(shape, dim):
    return lax.broadcasted_iota(jnp.int32, shape, dim)


def dot(a, b):
    return jnp.dot(a, b, preferred_element_type=F32)


def dot_t(a, b):
    return lax.dot_general(a, b, (((1,), (1,)), ((), ())), preferred_element_type=F32)


def far(i):
    return lax.rem(4 + jnp.where(lax.rem(i, 2) == 1, -((i + 1) // 2), i // 2) + 8, 8)


def peer(me, i):
    return lax.rem(me // 8 + far(i // 8), 8) * 8 + lax.rem(lax.rem(me, 8) + far(lax.rem(i, 8)), 8)


def halves(x):
    return jnp.concatenate([x[:8, :], x[8:, :]], axis=1)


def diagonal(d, mask):
    return jnp.sum(jnp.where(mask, d.reshape(64, 32, 64), 0.0), axis=0)


def kernel(*refs):
    names = NAMES
    h = dict(zip(names, refs))
    out_ref = refs[len(names)]
    local = [n for n in names if n not in ("lens", "mo", "eg", "ev", "rp")]
    rest = refs[len(names) + 1 :]
    v = dict(zip(local, rest))
    (
        wproj, moF, egF, evF, rpF, we, wt, rt, rpt, cio, cpi, msuf, s2,
        srcA, bufA, msgB, recvB, msgC, recvC, pairC, msgD, recvD, srcE, bufE, msgF, recvF,
        lsem, csem, xs, xr, ss, rs, ps, pr,
    ) = rest[len(local) :]
    me, tp = lax.axis_index("kv"), lax.axis_index("tp")
    first = tp == 0

    barrier = pltpu.get_barrier_semaphore()

    def greet(o, c):
        pl.semaphore_signal(
            barrier, inc=1, device_id={"kv": lax.rem(me + o, N)}, device_id_type=MESH
        )
        return c

    pl.semaphore_signal(barrier, inc=1, device_id={"tp": 1 - tp}, device_id_type=MESH)
    lax.fori_loop(1, N, greet, 0)

    loads = {n: pltpu.make_async_copy(h[n], v[n], lsem.at[i]) for i, n in enumerate(local)}
    shared = (("mo", moF), ("eg", egF), ("ev", evF), ("rp", rpF))
    mine = [pltpu.make_async_copy(h[n], f.at[tp], csem.at[i]) for i, (n, f) in enumerate(shared)]
    for c in loads.values():
        c.start()
    for c in mine:
        c.start()

    def send_all(p, source, target):
        def one(i, c):
            t = peer(me, i)
            pltpu.make_async_remote_copy(
                src_ref=source(t),
                dst_ref=target.at[me],
                send_sem=ss.at[p],
                recv_sem=rs.at[p],
                device_id={"kv": t},
                device_id_type=MESH,
            ).start()
            return c

        lax.fori_loop(0, N - 1, one, 0)

    def all_of(sem, buf):
        most = buf.at[pl.ds(0, N - 1)]
        pltpu.make_async_copy(most, most, sem).wait()

    def swap(p, source, target):
        return pltpu.make_async_remote_copy(
            src_ref=source,
            dst_ref=target,
            send_sem=ps.at[p],
            recv_sem=pr.at[p],
            device_id={"tp": 1 - tp},
            device_id_type=MESH,
        )

    for c in loads.values():
        c.wait()
    x_own = halves(v["hid"][...].astype(F32))
    srcA[...] = x_own.astype(BF16)
    bufA[tp, me] = x_own.astype(BF16)

    gain = v["mg"][...]
    wproj[0:32] = (v["gate"][...].astype(F32) * gain).astype(BF16)
    wproj[32:64] = (v["inner"][...].astype(F32) * gain).astype(BF16)
    wproj[64:80] = (v["inp"][...].astype(F32) * gain).astype(BF16)
    wproj[80:96] = (v["outp"][...].astype(F32) * gain).astype(BF16)
    wproj[96:128] = jnp.zeros((32, 2048), BF16)
    wproj[128:192] = (v["stepw"][...].astype(F32) * gain).astype(BF16)

    for a, (t, r) in enumerate((("tout", "rout"), ("tin", "rin"))):
        taps, rec = v[t][...], v[r][...].astype(F32)
        past = jnp.sum(rec * taps[:3], axis=0, keepdims=True)
        for g in range(8):
            at = slice(g * 128, (g + 1) * 128)
            cio[2 * a, g * 8 : (g + 1) * 8] = jnp.broadcast_to(past[:, at], (8, 128))
            cio[2 * a + 1, g * 8 : (g + 1) * 8] = jnp.broadcast_to(taps[3:4, at], (8, 128))
    taps, rec = v["tinner"], v["rinner"]
    cpi[...] = (
        taps[0] * rec[0].astype(F32) + taps[1] * rec[1].astype(F32) + taps[2] * rec[2].astype(F32)
    )

    live = (iota((64, 128), 1) < h["lens"][0]).astype(F32)
    masked = v["bdecay"][...] * live
    later = (iota((128, 128), 0) > iota((128, 128), 1)).astype(F32)
    msuf[...] = jnp.dot(
        masked, later, preferred_element_type=F32, precision=lax.Precision.HIGHEST
    )
    diag = iota((64, 64), 0) == iota((64, 64), 1)
    cached = jnp.sum(masked, axis=1, keepdims=True)
    cached_row = jnp.sum(jnp.where(diag, cached, 0.0), axis=0, keepdims=True)
    whole = v["states"][...]
    high = whole.astype(BF16)
    s2[:, 0:128] = high
    s2[:, 128:256] = (whole - high.astype(F32)).astype(BF16)

    pl.semaphore_wait(barrier, N)

    send_all(0, lambda t: srcA, bufA.at[tp])
    swaps = [
        pltpu.make_async_remote_copy(
            src_ref=h[n],
            dst_ref=f.at[tp],
            send_sem=xs.at[i],
            recv_sem=xr.at[i],
            device_id={"tp": 1 - tp},
            device_id_type=MESH,
        )
        for i, (n, f) in enumerate(shared)
    ]
    for c in swaps:
        c.start()
    for c in mine:
        c.wait()
    for c in swaps:
        c.wait()

    def own_rows(x):
        x = x.reshape(64, 2, 16, x.shape[-1])
        x = jnp.where(first, x[:, 0], x[:, 1])
        return x[:, :8].reshape(512, -1), x[:, 8:].reshape(512, -1)

    low, up = own_rows(
        jnp.concatenate([moF[0].astype(F32), moF[1].astype(F32)], axis=0).T
    )
    wt[...] = jnp.concatenate([low, up], axis=1).astype(BF16)
    gain2 = v["cg"][...]
    we[...] = jnp.zeros((192, 2048), BF16)
    rpt[...] = jnp.zeros((128, 2048), F32)
    for t in range(2):
        we[t * 48 : t * 48 + 44] = (egF[t].astype(F32) * gain2).astype(BF16)
        we[96 + t * 48 : 96 + t * 48 + 44] = (evF[t].astype(F32) * gain2).astype(BF16)
        rpt[t * 48 : t * 48 + 44] = rpF[t].astype(F32)
    low, up = own_rows(rpt[...].T)
    rt[:, 0:128] = low.astype(BF16)
    rt[:, 128:256] = up.astype(BF16)

    def gathered(p, src, buf):
        all_of(rs.at[p], buf.at[tp])
        c = swap(p, buf.at[tp], buf.at[tp])
        c.start()
        c.wait()
        x0, x1 = buf[0].astype(F32), buf[1].astype(F32)
        squares = jnp.sum(jnp.sum(x0 * x0 + x1 * x1, axis=0), axis=0, keepdims=True)
        squares = squares[:, 0:64] + squares[:, 64:128]
        rms = lax.rsqrt(squares / 2048.0 + EPS)
        full = jnp.concatenate(
            [x0[:, :, 0:64], x0[:, :, 64:128], x1[:, :, 0:64], x1[:, :, 64:128]], axis=1
        )
        return full.reshape(2048, 64).astype(BF16), rms

    x, rms = gathered(0, srcA, bufA)
    u = (dot(wproj[...], x) * rms).astype(BF16).astype(F32)
    by_seq = jnp.concatenate([u, jnp.zeros((64, 64), F32)], axis=0).T
    msgB[...] = by_seq[:, 0:128].reshape(64, 1, 128)
    recvB[me] = msgB[me]
    send_all(1, lambda t: msgB.at[t], recvB)

    step_pre = jnp.sum(
        jnp.where(iota((64, 64), 0) == me, by_seq[:, 128:192], 0.0), axis=0, keepdims=True
    )
    shifted = step_pre + v["bias"][...]
    step = jnp.maximum(shifted, 0.0) + jnp.log1p(jnp.exp(-jnp.abs(shifted)))
    decay = -jnp.exp(v["dlog"][...]) * step
    e_total = jnp.exp(decay + cached_row)
    decay_col = jnp.sum(jnp.where(diag, decay, 0.0), axis=1, keepdims=True)
    faded = live * jnp.exp(decay_col + msuf[...])

    n_of, k_of = iota((128, 256), 1), iota((128, 256), 0)
    base = jnp.where(n_of < 128, 80, 64)
    spread = ((k_of - base) == (n_of & 15)).astype(BF16)
    here = ((iota((64, 256), 1) & 127) >> 4) == (iota((64, 256), 0) & 7)
    group = ((iota((64, 64), 0) >> 3) == (iota((64, 64), 1) >> 3)).astype(BF16)
    own_head = iota((64, 32, 64), 0) == iota((64, 32, 64), 2)

    all_of(rs.at[1], recvB)
    heads = recvB[...].reshape(64, 128)
    placed = jnp.where(here, dot(heads.astype(BF16), spread), 0.0).astype(BF16)
    maps = dot(group, placed)
    readout = silu(cio[0] + cio[1] * maps[:, 0:128]).astype(BF16)
    conv_input = silu(cio[2] + cio[3] * maps[:, 128:256])
    readout_f = readout.astype(F32)
    own_score = jnp.sum(readout_f * conv_input, axis=1, keepdims=True)
    own_row = jnp.sum(jnp.where(diag, own_score, 0.0), axis=0, keepdims=True)
    of_group = iota((64, 128), 0) >> 3
    blocks = jnp.concatenate(
        [jnp.where(of_group == g, readout_f, 0.0) for g in range(8)], axis=1
    ).astype(BF16)
    score = dot_t(blocks, v["binput"][...])
    weight = (faded * score).astype(BF16)
    from_block = diagonal(dot_t(v["binner"][...], weight), own_head)
    twice = jnp.concatenate([readout, readout], axis=1)
    from_state = diagonal(dot_t(s2[...], twice), own_head)
    by_channel = heads.T
    conv_inner = silu(cpi[...] + v["tinner"][3] * by_channel[32:64])
    mix = from_block + e_total * from_state + (own_row * step + v["skip"][...]) * conv_inner
    raw = mix * silu(by_channel[0:32])
    squares = jnp.sum(jnp.sum(raw * raw, axis=1, keepdims=True), axis=0, keepdims=True)
    gated = (raw * v["normg"][...]).astype(BF16).astype(F32)
    out_c = jnp.concatenate(
        [
            jnp.where(first, gated, 0.0),
            jnp.where(first, 0.0, gated),
            jnp.where(iota((8, 64), 0) == tp, squares, 0.0),
            jnp.zeros((56, 64), F32),
        ],
        axis=0,
    )
    msgC[...] = out_c.T.reshape(64, 1, 128)
    recvC[me] = msgC[me]
    send_all(2, lambda t: msgC.at[t], recvC)

    all_of(rs.at[2], recvC)
    c = swap(2, recvC, pairC)
    c.start()
    c.wait()
    g = (recvC[...] + pairC[...]).reshape(64, 128).T
    rms_gate = lax.rsqrt((g[64:65] + g[65:66]) / 4096.0 + EPS)
    zero = jnp.zeros((64, 64), F32)
    gg = jnp.concatenate(
        [jnp.concatenate([g[0:64], zero], axis=1), jnp.concatenate([zero, g[0:64]], axis=1)],
        axis=0,
    ).astype(BF16)
    rms2 = jnp.concatenate([rms_gate, rms_gate], axis=1)
    msgD[...] = (dot(wt[...], gg) * rms2).astype(BF16).reshape(64, 8, 128)
    recvD[me] = msgD[me]
    send_all(3, lambda t: msgD.at[t], recvD)
    all_of(rs.at[3], recvD)
    mid = (x_own + jnp.sum(recvD[...].astype(F32), axis=0)).astype(BF16)
    srcE[...] = mid
    bufE[tp, me] = mid
    send_all(4, lambda t: srcE, bufE.at[tp])
    y, rms = gathered(4, srcE, bufE)
    u = dot(we[...], y) * rms
    act = silu(u[0:96]) * u[96:192]
    zero = jnp.zeros((96, 64), F32)
    pad = jnp.zeros((32, 128), F32)
    aa = jnp.concatenate(
        [
            jnp.concatenate([act, zero], axis=1),
            pad,
            jnp.concatenate([zero, act], axis=1),
            pad,
        ],
        axis=0,
    ).astype(BF16)
    msgF[...] = dot(rt[...], aa).astype(BF16).reshape(64, 8, 128)
    recvF[me] = msgF[me]
    send_all(5, lambda t: msgF.at[t], recvF)
    all_of(rs.at[5], recvF)
    end = mid.astype(F32) + jnp.sum(recvF[...].astype(F32), axis=0)
    out_ref[...] = jnp.concatenate([end[:, 0:64], end[:, 64:128]], axis=0).astype(BF16)
    for p, b in ((0, bufA.at[0]), (1, recvB), (2, recvC), (3, recvD), (4, bufE.at[0]), (5, recvF)):
        all_of(ss.at[p], b)


def shards(
    hidden, mixer_gain, gate_proj, inner_proj, input_proj, output_proj, step_proj, step_bias,
    decay_log, skip_gain, taps_inner, taps_input, taps_output, recent_inner, recent_input,
    recent_output, states, block_inner, block_input, block_decay, lengths, norm_gain, mixer_out,
    channel_gain, expand_gate, expand_value, reduce_proj,
):
    args = dict(
        hid=hidden,
        mg=mixer_gain.reshape(1, 2048),
        gate=gate_proj.transpose(1, 2, 0).reshape(32, 2048),
        inner=inner_proj.transpose(1, 2, 0).reshape(32, 2048),
        inp=input_proj.T,
        outp=output_proj.T,
        stepw=step_proj.T,
        bias=step_bias.reshape(1, 64),
        dlog=decay_log.reshape(1, 64),
        skip=skip_gain.reshape(1, 64),
        tinner=taps_inner.transpose(0, 2, 1),
        tin=taps_input,
        tout=taps_output,
        rinner=recent_inner.transpose(0, 1, 3, 2).reshape(3, 32, 64),
        rin=recent_input.reshape(3, 1024),
        rout=recent_output.reshape(3, 1024),
        states=states.reshape(2048, 128),
        binner=block_inner.transpose(0, 2, 3, 1).reshape(2048, 128),
        binput=block_input.reshape(128, 1024),
        bdecay=block_decay.transpose(0, 2, 1).reshape(64, 128),
        lens=lengths,
        normg=norm_gain.T,
        mo=mixer_out.reshape(32, 2048),
        cg=channel_gain.reshape(1, 2048),
        eg=expand_gate.T,
        ev=expand_value.T,
        rp=reduce_proj,
    )
    away = ("lens", "mo", "eg", "ev", "rp")
    near = [pltpu.VMEM(a.shape, a.dtype) for n, a in args.items() if n not in away]
    scratch = near + [
        pltpu.VMEM((192, 2048), BF16),
        pltpu.VMEM((2, 32, 2048), BF16),
        pltpu.VMEM((2, 44, 2048), BF16),
        pltpu.VMEM((2, 44, 2048), BF16),
        pltpu.VMEM((2, 44, 2048), BF16),
        pltpu.VMEM((192, 2048), BF16),
        pltpu.VMEM((512, 128), BF16),
        pltpu.VMEM((512, 256), BF16),
        pltpu.VMEM((128, 2048), F32),
        pltpu.VMEM((4, 64, 128), F32),
        pltpu.VMEM((32, 64), F32),
        pltpu.VMEM((64, 128), F32),
        pltpu.VMEM((2048, 256), BF16),
        pltpu.VMEM((8, 128), BF16),
        pltpu.VMEM((2, N, 8, 128), BF16),
        pltpu.VMEM((N, 1, 128), F32),
        pltpu.VMEM((N, 1, 128), F32),
        pltpu.VMEM((N, 1, 128), F32),
        pltpu.VMEM((N, 1, 128), F32),
        pltpu.VMEM((N, 1, 128), F32),
        pltpu.VMEM((N, 8, 128), BF16),
        pltpu.VMEM((N, 8, 128), BF16),
        pltpu.VMEM((8, 128), BF16),
        pltpu.VMEM((2, N, 8, 128), BF16),
        pltpu.VMEM((N, 8, 128), BF16),
        pltpu.VMEM((N, 8, 128), BF16),
        pltpu.SemaphoreType.DMA((len(near),)),
        pltpu.SemaphoreType.DMA((4,)),
        pltpu.SemaphoreType.DMA((4,)),
        pltpu.SemaphoreType.DMA((4,)),
        pltpu.SemaphoreType.DMA((6,)),
        pltpu.SemaphoreType.DMA((6,)),
        pltpu.SemaphoreType.DMA((6,)),
        pltpu.SemaphoreType.DMA((6,)),
    ]
    space = [
        pl.BlockSpec(memory_space=pltpu.SMEM if n == "lens" else pl.ANY) for n in args
    ]
    return pl.pallas_call(
        kernel,
        out_shape=jax.ShapeDtypeStruct((16, 64), BF16),
        in_specs=space,
        out_specs=pl.BlockSpec(memory_space=pltpu.VMEM),
        scratch_shapes=scratch,
        compiler_params=pltpu.CompilerParams(collective_id=0, has_side_effects=True),
    )(*args.values())


def solution(mesh):
    in_specs = (
        P(KV_TP, "dp"),
        P(),
        P(None, "kv", "tp"),
        P(None, "kv", "tp"),
        P(None, "kv"),
        P(None, "kv"),
        P(),
        P(),
        P(),
        P(),
        P(None, None, "tp"),
        P(),
        P(),
        P(DP_KV, None, None, "tp"),
        P(DP_KV, None, None),
        P(DP_KV, None, None),
        P(DP_KV, None, "tp", None),
        P(DP_KV, None, None, "tp"),
        P(DP_KV, None, None),
        P(DP_KV, None, None),
        P(DP_KV),
        P(None, "tp"),
        P("kv", "tp", None),
        P(),
        P(None, KV_TP),
        P(None, KV_TP),
        P(KV_TP, None),
    )
    return jax.shard_map(
        shards, mesh=mesh, in_specs=in_specs, out_specs=P(KV_TP, "dp"), check_vma=False
    )
```

```python
import jax
import jax.numpy as jnp
from jax import lax
from jax.experimental import pallas as pl
from jax.experimental.pallas import tpu as pltpu
from jax.sharding import PartitionSpec as P

F32 = jnp.float32
BF16 = jnp.bfloat16
MESH = pl.DeviceIdType.MESH
EPS = 1e-05
N = 64
DP_KV = ("dp", "kv")
KV_TP = ("kv", "tp")
NAMES = (
    "hid",
    "mg",
    "gate",
    "inner",
    "inp",
    "outp",
    "stepw",
    "bias",
    "dlog",
    "skip",
    "tinner",
    "tin",
    "tout",
    "rinner",
    "rin",
    "rout",
    "states",
    "binner",
    "binput",
    "bdecay",
    "lens",
    "normg",
    "mo",
    "cg",
    "eg",
    "ev",
    "rp",
)


def silu(v):
    return v / (1.0 + jnp.exp(-v))


def iota(shape, dim):
    return lax.broadcasted_iota(jnp.int32, shape, dim)


def dot(a, b):
    return jnp.dot(a, b, preferred_element_type=F32)


def dot_t(a, b):
    return lax.dot_general(a, b, (((1,), (1,)), ((), ())), preferred_element_type=F32)


def far(i):
    return lax.rem(4 + jnp.where(lax.rem(i, 2) == 1, -((i + 1) // 2), i // 2) + 8, 8)


def peer(me, i):
    return lax.rem(me // 8 + far(i // 8), 8) * 8 + lax.rem(lax.rem(me, 8) + far(lax.rem(i, 8)), 8)


def halves(x):
    return jnp.concatenate([x[:8, :], x[8:, :]], axis=1)


def diagonal(d, mask):
    return jnp.sum(jnp.where(mask, d.reshape(64, 32, 64), 0.0), axis=0)


def kernel(*refs):
    names = NAMES
    h = dict(zip(names, refs))
    out_ref = refs[len(names)]
    local = [n for n in names if n not in ("eg", "ev", "rp")]
    rest = refs[len(names) + 1 :]
    v = dict(zip(local, rest))
    (
        wproj, egF, evF, rpF, we, wd, rt, rpt, cio, cpi, msuf, s2, gf,
        srcA, bufA, msgB, recvB, srcC, recvC, sumC, pairC, msgW, recvW, srcE, bufE, msgF, recvF,
        lsem, csem, xs, xr, ss, rs, ps, pr,
    ) = rest[len(local) :]
    me, tp = lax.axis_index("kv"), lax.axis_index("tp")
    first = tp == 0

    barrier = pltpu.get_barrier_semaphore()

    def greet(o, c):
        pl.semaphore_signal(
            barrier, inc=1, device_id={"kv": lax.rem(me + o, N)}, device_id_type=MESH
        )
        return c

    pl.semaphore_signal(barrier, inc=1, device_id={"tp": 1 - tp}, device_id_type=MESH)
    lax.fori_loop(1, N, greet, 0)

    loads = {n: pltpu.make_async_copy(h[n], v[n], lsem.at[i]) for i, n in enumerate(local)}
    shared = (("eg", egF), ("ev", evF), ("rp", rpF))
    mine = [pltpu.make_async_copy(h[n], f.at[tp], csem.at[i]) for i, (n, f) in enumerate(shared)]
    for c in loads.values():
        c.start()
    for c in mine:
        c.start()

    def send_all(p, source, target):
        def one(i, c):
            t = peer(me, i)
            pltpu.make_async_remote_copy(
                src_ref=source(t),
                dst_ref=target.at[me],
                send_sem=ss.at[p],
                recv_sem=rs.at[p],
                device_id={"kv": t},
                device_id_type=MESH,
            ).start()
            return c

        lax.fori_loop(0, N - 1, one, 0)

    def all_of(sem, buf):
        most = buf.at[pl.ds(0, N - 1)]
        pltpu.make_async_copy(most, most, sem).wait()

    def swap(p, source, target):
        return pltpu.make_async_remote_copy(
            src_ref=source,
            dst_ref=target,
            send_sem=ps.at[p],
            recv_sem=pr.at[p],
            device_id={"tp": 1 - tp},
            device_id_type=MESH,
        )

    for c in loads.values():
        c.wait()
    x_own = halves(v["hid"][...].astype(F32))
    srcA[...] = x_own.astype(BF16)
    bufA[tp, me] = x_own.astype(BF16)

    gain = v["mg"][...]
    wproj[0:32] = (v["gate"][...].astype(F32) * gain).astype(BF16)
    wproj[32:64] = (v["inner"][...].astype(F32) * gain).astype(BF16)
    wproj[64:80] = (v["inp"][...].astype(F32) * gain).astype(BF16)
    wproj[80:96] = (v["outp"][...].astype(F32) * gain).astype(BF16)
    wproj[96:128] = jnp.zeros((32, 2048), BF16)
    wproj[128:192] = (v["stepw"][...].astype(F32) * gain).astype(BF16)

    for a, (t, r) in enumerate((("tout", "rout"), ("tin", "rin"))):
        taps, rec = v[t][...], v[r][...].astype(F32)
        past = jnp.sum(rec * taps[:3], axis=0, keepdims=True)
        for g in range(8):
            at = slice(g * 128, (g + 1) * 128)
            cio[2 * a, g * 8 : (g + 1) * 8] = jnp.broadcast_to(past[:, at], (8, 128))
            cio[2 * a + 1, g * 8 : (g + 1) * 8] = jnp.broadcast_to(taps[3:4, at], (8, 128))
    taps, rec = v["tinner"], v["rinner"]
    cpi[...] = (
        taps[0] * rec[0].astype(F32) + taps[1] * rec[1].astype(F32) + taps[2] * rec[2].astype(F32)
    )

    live = (iota((64, 128), 1) < v["lens"][0:1, 0:1]).astype(F32)
    masked = v["bdecay"][...] * live
    later = (iota((128, 128), 0) > iota((128, 128), 1)).astype(F32)
    msuf[...] = jnp.dot(
        masked, later, preferred_element_type=F32, precision=lax.Precision.HIGHEST
    )
    diag = iota((64, 64), 0) == iota((64, 64), 1)
    cached = jnp.sum(masked, axis=1, keepdims=True)
    cached_row = jnp.sum(jnp.where(diag, cached, 0.0), axis=0, keepdims=True)
    whole = v["states"][...]
    high = whole.astype(BF16)
    s2[:, 0:128] = high
    s2[:, 128:256] = (whole - high.astype(F32)).astype(BF16)

    lane = iota((32, 64), 1)
    norm = jnp.sum(jnp.where(lane == me, v["normg"][...], 0.0), axis=1, keepdims=True)
    rows = jnp.concatenate([v["mo"][...].astype(F32) * norm, jnp.zeros((96, 2048), F32)], axis=0)
    rows = rows.T.reshape(64, 4, 8, 128)
    packed = rows[:, 0].reshape(512, 128)
    for q in range(1, 4):
        packed = packed + pltpu.roll(rows[:, q].reshape(512, 128), 32 * q, 1)
    msgW[...] = packed.astype(BF16).reshape(64, 8, 128)
    recvW[me] = msgW[me]

    pl.semaphore_wait(barrier, N)

    send_all(0, lambda t: srcA, bufA.at[tp])
    swaps = [
        pltpu.make_async_remote_copy(
            src_ref=h[n],
            dst_ref=f.at[tp],
            send_sem=xs.at[i],
            recv_sem=xr.at[i],
            device_id={"tp": 1 - tp},
            device_id_type=MESH,
        )
        for i, (n, f) in enumerate(shared)
    ]
    for c in swaps:
        c.start()
    for c in mine:
        c.wait()
    for c in swaps:
        c.wait()

    def own_rows(x):
        x = x.reshape(64, 2, 16, x.shape[-1])
        x = jnp.where(first, x[:, 0], x[:, 1])
        return x[:, :8].reshape(512, -1), x[:, 8:].reshape(512, -1)

    gain2 = v["cg"][...]
    we[...] = jnp.zeros((192, 2048), BF16)
    rpt[...] = jnp.zeros((128, 2048), F32)
    for t in range(2):
        we[t * 48 : t * 48 + 44] = (egF[t].astype(F32) * gain2).astype(BF16)
        we[96 + t * 48 : 96 + t * 48 + 44] = (evF[t].astype(F32) * gain2).astype(BF16)
        rpt[t * 48 : t * 48 + 44] = rpF[t].astype(F32)
    low, up = own_rows(rpt[...].T)
    rt[:, 0:128] = low.astype(BF16)
    rt[:, 128:256] = up.astype(BF16)

    def gathered(p, src, buf):
        all_of(rs.at[p], buf.at[tp])
        c = swap(p, buf.at[tp], buf.at[tp])
        c.start()
        c.wait()
        x0, x1 = buf[0].astype(F32), buf[1].astype(F32)
        squares = jnp.sum(jnp.sum(x0 * x0 + x1 * x1, axis=0), axis=0, keepdims=True)
        squares = squares[:, 0:64] + squares[:, 64:128]
        rms = lax.rsqrt(squares / 2048.0 + EPS)
        full = jnp.concatenate(
            [x0[:, :, 0:64], x0[:, :, 64:128], x1[:, :, 0:64], x1[:, :, 64:128]], axis=1
        )
        return full.reshape(2048, 64).astype(BF16), rms

    x, rms = gathered(0, srcA, bufA)
    u = (dot(wproj[...], x) * rms).astype(BF16).astype(F32)
    by_seq = jnp.concatenate([u, jnp.zeros((64, 64), F32)], axis=0).T
    msgB[...] = by_seq[:, 0:128].reshape(64, 1, 128)
    recvB[me] = msgB[me]
    send_all(1, lambda t: msgB.at[t], recvB)
    send_all(3, lambda t: msgW.at[t], recvW)

    step_pre = jnp.sum(
        jnp.where(iota((64, 64), 0) == me, by_seq[:, 128:192], 0.0), axis=0, keepdims=True
    )
    shifted = step_pre + v["bias"][...]
    step = jnp.maximum(shifted, 0.0) + jnp.log1p(jnp.exp(-jnp.abs(shifted)))
    decay = -jnp.exp(v["dlog"][...]) * step
    e_total = jnp.exp(decay + cached_row)
    decay_col = jnp.sum(jnp.where(diag, decay, 0.0), axis=1, keepdims=True)
    faded = live * jnp.exp(decay_col + msuf[...])

    n_of, k_of = iota((128, 256), 1), iota((128, 256), 0)
    base = jnp.where(n_of < 128, 80, 64)
    spread = ((k_of - base) == (n_of & 15)).astype(BF16)
    here = ((iota((64, 256), 1) & 127) >> 4) == (iota((64, 256), 0) & 7)
    group = ((iota((64, 64), 0) >> 3) == (iota((64, 64), 1) >> 3)).astype(BF16)
    own_head = iota((64, 32, 64), 0) == iota((64, 32, 64), 2)

    all_of(rs.at[1], recvB)
    heads = recvB[...].reshape(64, 128)
    placed = jnp.where(here, dot(heads.astype(BF16), spread), 0.0).astype(BF16)
    maps = dot(group, placed)
    readout = silu(cio[0] + cio[1] * maps[:, 0:128]).astype(BF16)
    conv_input = silu(cio[2] + cio[3] * maps[:, 128:256])
    readout_f = readout.astype(F32)
    own_score = jnp.sum(readout_f * conv_input, axis=1, keepdims=True)
    own_row = jnp.sum(jnp.where(diag, own_score, 0.0), axis=0, keepdims=True)
    of_group = iota((64, 128), 0) >> 3
    blocks = jnp.concatenate(
        [jnp.where(of_group == g, readout_f, 0.0) for g in range(8)], axis=1
    ).astype(BF16)
    score = dot_t(blocks, v["binput"][...])
    weight = (faded * score).astype(BF16)
    from_block = diagonal(dot_t(v["binner"][...], weight), own_head)
    twice = jnp.concatenate([readout, readout], axis=1)
    from_state = diagonal(dot_t(s2[...], twice), own_head)
    by_channel = heads.T
    conv_inner = silu(cpi[...] + v["tinner"][3] * by_channel[32:64])
    mix = from_block + e_total * from_state + (own_row * step + v["skip"][...]) * conv_inner
    raw = mix * silu(by_channel[0:32])
    by_head = jnp.concatenate([raw, jnp.zeros((96, 64), F32)], axis=0).T
    packed = by_head[0:16]
    for q in range(1, 4):
        packed = packed + pltpu.roll(by_head[q * 16 : (q + 1) * 16], 32 * q, 1)
    srcC[...] = packed.astype(BF16)
    recvC[me] = packed.astype(BF16)
    send_all(2, lambda t: srcC, recvC)

    all_of(rs.at[3], recvW)
    tiles = recvW[...].astype(F32).reshape(4, 128, 128)
    block = iota((128, 128), 1) >> 5
    for dd in range(4):
        out = jnp.zeros((128, 128), F32)
        for q in range(4):
            turned = tiles[q] if q == dd else pltpu.roll(tiles[q], (32 * (q - dd)) % 128, 1)
            out = jnp.where(block == q, turned, out)
        out = out.astype(BF16).reshape(16, 8, 128)
        for i in range(16):
            wd[i // 2, dd * 8 : dd * 8 + 8, (i % 2) * 128 : (i % 2) * 128 + 128] = out[i]

    all_of(rs.at[2], recvC)
    gates = recvC[...].astype(F32)
    gf[...] = gates.reshape(1024, 128)
    partial = jnp.zeros((32, 64), F32)
    for i in range(8):
        pair = [gf[pl.ds(2 * i + e, 64, stride=16), :] for e in range(2)]
        partial = partial + dot_t(wd[i], jnp.concatenate(pair, axis=1).astype(BF16))
    squares = jnp.sum(jnp.sum(gates * gates, axis=1), axis=1, keepdims=True)
    squares = jnp.sum(jnp.where(diag, squares, 0.0), axis=0, keepdims=True)
    squares = jnp.broadcast_to(jnp.concatenate([squares, squares], axis=1), (8, 128))
    part0, part1 = halves(partial[0:16]), halves(partial[16:32])
    sumC[0:8] = jnp.where(first, part1, part0)
    sumC[8:16] = squares
    c = swap(2, sumC, pairC)
    c.start()
    c.wait()
    mixed = jnp.where(first, part0, part1) + pairC[0:8]
    mixed = mixed * lax.rsqrt((squares + pairC[8:16]) / 4096.0 + EPS)
    mid = (x_own + mixed).astype(BF16)
    srcE[...] = mid
    bufE[tp, me] = mid
    send_all(4, lambda t: srcE, bufE.at[tp])
    y, rms = gathered(4, srcE, bufE)
    u = dot(we[...], y) * rms
    act = silu(u[0:96]) * u[96:192]
    zero = jnp.zeros((96, 64), F32)
    pad = jnp.zeros((32, 128), F32)
    aa = jnp.concatenate(
        [
            jnp.concatenate([act, zero], axis=1),
            pad,
            jnp.concatenate([zero, act], axis=1),
            pad,
        ],
        axis=0,
    ).astype(BF16)
    msgF[...] = dot(rt[...], aa).astype(BF16).reshape(64, 8, 128)
    recvF[me] = msgF[me]
    send_all(5, lambda t: msgF.at[t], recvF)
    all_of(rs.at[5], recvF)
    end = mid.astype(F32) + jnp.sum(recvF[...].astype(F32), axis=0)
    out_ref[...] = jnp.concatenate([end[:, 0:64], end[:, 64:128]], axis=0)
    for p, b in ((0, bufA.at[0]), (1, recvB), (2, recvC), (3, recvW), (4, bufE.at[0]), (5, recvF)):
        all_of(ss.at[p], b)


def shards(
    hidden, mixer_gain, gate_proj, inner_proj, input_proj, output_proj, step_proj, step_bias,
    decay_log, skip_gain, taps_inner, taps_input, taps_output, recent_inner, recent_input,
    recent_output, states, block_inner, block_input, block_decay, lengths, norm_gain, mixer_out,
    channel_gain, expand_gate, expand_value, reduce_proj,
):
    args = dict(
        hid=hidden,
        mg=mixer_gain.reshape(1, 2048),
        gate=gate_proj.transpose(1, 2, 0).reshape(32, 2048),
        inner=inner_proj.transpose(1, 2, 0).reshape(32, 2048),
        inp=input_proj.T,
        outp=output_proj.T,
        stepw=step_proj.T,
        bias=step_bias.reshape(1, 64),
        dlog=decay_log.reshape(1, 64),
        skip=skip_gain.reshape(1, 64),
        tinner=taps_inner.transpose(0, 2, 1),
        tin=taps_input,
        tout=taps_output,
        rinner=recent_inner.transpose(0, 1, 3, 2).reshape(3, 32, 64),
        rin=recent_input.reshape(3, 1024),
        rout=recent_output.reshape(3, 1024),
        states=states.reshape(2048, 128),
        binner=block_inner.transpose(0, 2, 3, 1).reshape(2048, 128),
        binput=block_input.reshape(128, 1024),
        bdecay=block_decay.transpose(0, 2, 1).reshape(64, 128),
        lens=lengths.reshape(1, 1),
        normg=norm_gain.T,
        mo=mixer_out.reshape(32, 2048),
        cg=channel_gain.reshape(1, 2048),
        eg=expand_gate.T,
        ev=expand_value.T,
        rp=reduce_proj,
    )
    away = ("eg", "ev", "rp")
    near = [
        pltpu.VMEM(a.shape, a.dtype)
        for n, a in args.items()
        if n not in away
    ]
    scratch = near + [
        pltpu.VMEM((192, 2048), BF16),
        pltpu.VMEM((2, 44, 2048), BF16),
        pltpu.VMEM((2, 44, 2048), BF16),
        pltpu.VMEM((2, 44, 2048), BF16),
        pltpu.VMEM((192, 2048), BF16),
        pltpu.VMEM((8, 32, 256), BF16),
        pltpu.VMEM((512, 256), BF16),
        pltpu.VMEM((128, 2048), F32),
        pltpu.VMEM((4, 64, 128), F32),
        pltpu.VMEM((32, 64), F32),
        pltpu.VMEM((64, 128), F32),
        pltpu.VMEM((2048, 256), BF16),
        pltpu.VMEM((1024, 128), F32),
        pltpu.VMEM((8, 128), BF16),
        pltpu.VMEM((2, N, 8, 128), BF16),
        pltpu.VMEM((N, 1, 128), F32),
        pltpu.VMEM((N, 1, 128), F32),
        pltpu.VMEM((16, 128), BF16),
        pltpu.VMEM((N, 16, 128), BF16),
        pltpu.VMEM((16, 128), F32),
        pltpu.VMEM((16, 128), F32),
        pltpu.VMEM((N, 8, 128), BF16),
        pltpu.VMEM((N, 8, 128), BF16),
        pltpu.VMEM((8, 128), BF16),
        pltpu.VMEM((2, N, 8, 128), BF16),
        pltpu.VMEM((N, 8, 128), BF16),
        pltpu.VMEM((N, 8, 128), BF16),
        pltpu.SemaphoreType.DMA((len(near),)),
        pltpu.SemaphoreType.DMA((3,)),
        pltpu.SemaphoreType.DMA((3,)),
        pltpu.SemaphoreType.DMA((3,)),
        pltpu.SemaphoreType.DMA((6,)),
        pltpu.SemaphoreType.DMA((6,)),
        pltpu.SemaphoreType.DMA((6,)),
        pltpu.SemaphoreType.DMA((6,)),
    ]
    space = [
        pl.BlockSpec(memory_space=pltpu.HBM if n == "lens" else pl.ANY) for n in args
    ]
    end = pl.pallas_call(
        kernel,
        out_shape=pltpu.VMEM((16, 64), F32),
        in_specs=space,
        out_specs=pl.BlockSpec(memory_space=pltpu.VMEM),
        scratch_shapes=scratch,
        compiler_params=pltpu.CompilerParams(collective_id=0, has_side_effects=True),
    )(*args.values())
    return end.astype(BF16)


def solution(mesh):
    in_specs = (
        P(KV_TP, "dp"),
        P(),
        P(None, "kv", "tp"),
        P(None, "kv", "tp"),
        P(None, "kv"),
        P(None, "kv"),
        P(),
        P(),
        P(),
        P(),
        P(None, None, "tp"),
        P(),
        P(),
        P(DP_KV, None, None, "tp"),
        P(DP_KV, None, None),
        P(DP_KV, None, None),
        P(DP_KV, None, "tp", None),
        P(DP_KV, None, None, "tp"),
        P(DP_KV, None, None),
        P(DP_KV, None, None),
        P(DP_KV),
        P(None, "tp"),
        P("kv", "tp", None),
        P(),
        P(None, KV_TP),
        P(None, KV_TP),
        P(KV_TP, None),
    )
    return jax.shard_map(
        shards, mesh=mesh, in_specs=in_specs, out_specs=P(KV_TP, "dp"), check_vma=False
    )
```

```python
import jax
import jax.numpy as jnp
from jax import lax
from jax.experimental import pallas as pl
from jax.experimental.pallas import tpu as pltpu
from jax.sharding import PartitionSpec as P

F32 = jnp.float32
BF16 = jnp.bfloat16
MESH = pl.DeviceIdType.MESH
EPS = 1e-05
N = 64
DP_KV = ("dp", "kv")
KV_TP = ("kv", "tp")
NAMES = (
    "hid",
    "mg",
    "gate",
    "inner",
    "inp",
    "outp",
    "stepw",
    "bias",
    "dlog",
    "skip",
    "tinner",
    "tin",
    "tout",
    "rinner",
    "rin",
    "rout",
    "states",
    "binner",
    "binput",
    "bdecay",
    "lens",
    "normg",
    "mo",
    "cg",
    "eg",
    "ev",
    "rp",
)


def silu(v):
    return v / (1.0 + jnp.exp(-v))


def iota(shape, dim):
    return lax.broadcasted_iota(jnp.int32, shape, dim)


def dot(a, b):
    return jnp.dot(a, b, preferred_element_type=F32)


def dot_t(a, b):
    return lax.dot_general(a, b, (((1,), (1,)), ((), ())), preferred_element_type=F32)


def halves(x):
    return jnp.concatenate([x[:8, :], x[8:, :]], axis=1)


def diagonal(d, mask):
    return jnp.sum(jnp.where(mask, d.reshape(64, 32, 64), 0.0), axis=0)


def kernel(*refs):
    names = NAMES
    h = dict(zip(names, refs))
    out_ref = refs[len(names)]
    local = [n for n in names if n not in ("gate", "inner", "eg", "ev", "rp")]
    rest = refs[len(names) + 1 :]
    v = dict(zip(local, rest))
    (
        wfull, wproj, giF, egF, evF, rpF, we, we2, wd, rt, rpt, cio, cpi, msuf, s2, gf,
        srcA, bufA, msgB, recvB, sumA, pairA, sumE, pairE, srcC, recvC, sumC, pairC, msgW, recvW, srcE, bufE, msgF, recvF,
        lsem, csem, xs, xr, ss, rs, ps, pr,
    ) = rest[len(local) :]
    me, tp = lax.axis_index("kv"), lax.axis_index("tp")
    first = tp == 0

    order = (4, 3, 5, 2, 6, 1, 7, 0)
    in_rows = [lax.rem(me // 8 + o, 8) * 8 for o in order]
    in_cols = [lax.rem(lax.rem(me, 8) + o, 8) for o in order]
    peers = [r + c for r in in_rows for c in in_cols][: N - 1]
    dist = [min(o, 8 - o) for o in order]
    ranks = sorted(range(N - 1), key=lambda i: -(dist[i // 8] + dist[i % 8]))
    peers = [peers[i] for i in ranks]

    barrier = pltpu.get_barrier_semaphore()

    pl.semaphore_signal(barrier, inc=1, device_id={"tp": 1 - tp}, device_id_type=MESH)
    for t in peers:
        pl.semaphore_signal(barrier, inc=1, device_id={"kv": t}, device_id_type=MESH)

    loads = {n: pltpu.make_async_copy(h[n], v[n], lsem.at[i]) for i, n in enumerate(local)}
    shared = (
        ("gate", giF.at[tp, pl.ds(0, 32)]),
        ("inner", giF.at[tp, pl.ds(32, 32)]),
        ("eg", egF.at[tp]),
        ("ev", evF.at[tp]),
        ("rp", rpF.at[tp]),
    )
    mine = [pltpu.make_async_copy(h[n], f, csem.at[i]) for i, (n, f) in enumerate(shared)]
    for c in loads.values():
        c.start()
    for c in mine:
        c.start()

    def send_all(p, source, target):
        def one(i, c):
            t = i
            pltpu.make_async_remote_copy(
                src_ref=source(t),
                dst_ref=target.at[me],
                send_sem=ss.at[p],
                recv_sem=rs.at[p],
                device_id={"kv": t},
                device_id_type=MESH,
            ).start()
            return c

        for t in peers:
            one(t, 0)

    def all_of(sem, buf):
        most = buf.at[pl.ds(0, N - 1)]
        pltpu.make_async_copy(most, most, sem).wait()

    def swap(p, source, target):
        return pltpu.make_async_remote_copy(
            src_ref=source,
            dst_ref=target,
            send_sem=ps.at[p],
            recv_sem=pr.at[p],
            device_id={"tp": 1 - tp},
            device_id_type=MESH,
        )

    loads["hid"].wait()
    x_own = halves(v["hid"][...].astype(F32))
    srcA[...] = x_own.astype(BF16)
    bufA[me] = x_own.astype(BF16)
    pl.semaphore_wait(barrier, N)

    send_all(0, lambda t: srcA, bufA)
    swaps = [
        pltpu.make_async_remote_copy(
            src_ref=h[n],
            dst_ref=f,
            send_sem=xs.at[i],
            recv_sem=xr.at[i],
            device_id={"tp": 1 - tp},
            device_id_type=MESH,
        )
        for i, (n, f) in enumerate(shared)
    ]
    for c in swaps:
        c.start()
    for n in local:
        if n != "hid":
            loads[n].wait()

    gain = v["mg"][...]
    wfull[128:144] = (v["inp"][...].astype(F32) * gain).astype(BF16)
    wfull[144:160] = (v["outp"][...].astype(F32) * gain).astype(BF16)
    wfull[160:224] = (v["stepw"][...].astype(F32) * gain).astype(BF16)
    low_lanes = iota((1, 128), 1) < 64
    to, at = iota((512, 256), 0), iota((512, 256), 1)
    spot = ((at & 127) >> 3) * 32 + 16 * tp + (at >> 7) * 8 + (at & 7)
    picked = (to == spot).astype(BF16)

    def pick(whole, out):
        n = whole.shape[0]
        for i in range(4):
            y = dot(whole[:, i * 512 : (i + 1) * 512], picked).astype(BF16)
            out[0:n, i * 128 : (i + 1) * 128] = y[:, 0:128]
            out[n : 2 * n, i * 128 : (i + 1) * 128] = y[:, 128:256]

    for c in mine[:2]:
        c.wait()
    for c in swaps[:2]:
        c.wait()
    for t in range(2):
        wfull[t * 64 : t * 64 + 64] = (giF[t].astype(F32) * gain).astype(BF16)
    pick(wfull, wproj)

    for a, (t, r) in enumerate((("tout", "rout"), ("tin", "rin"))):
        taps, rec = v[t][...], v[r][...].astype(F32)
        past = jnp.sum(rec * taps[:3], axis=0, keepdims=True)
        for g in range(8):
            at = slice(g * 128, (g + 1) * 128)
            cio[2 * a, g * 8 : (g + 1) * 8] = jnp.broadcast_to(past[:, at], (8, 128))
            cio[2 * a + 1, g * 8 : (g + 1) * 8] = jnp.broadcast_to(taps[3:4, at], (8, 128))
    taps, rec = v["tinner"], v["rinner"]
    cpi[...] = (
        taps[0] * rec[0].astype(F32) + taps[1] * rec[1].astype(F32) + taps[2] * rec[2].astype(F32)
    )

    live = (iota((64, 128), 1) < v["lens"][0:1, 0:1]).astype(F32)
    masked = v["bdecay"][...] * live
    later = (iota((128, 128), 0) > iota((128, 128), 1)).astype(F32)
    msuf[...] = jnp.dot(
        masked, later, preferred_element_type=F32, precision=lax.Precision.HIGHEST
    )
    diag = iota((64, 64), 0) == iota((64, 64), 1)
    cached = jnp.sum(masked, axis=1, keepdims=True)
    cached_row = jnp.sum(jnp.where(diag, cached, 0.0), axis=0, keepdims=True)
    whole = v["states"][...]
    high = whole.astype(BF16)
    s2[:, 0:128] = high
    s2[:, 128:256] = (whole - high.astype(F32)).astype(BF16)

    lane = iota((32, 64), 1)
    norm = jnp.sum(jnp.where(lane == me, v["normg"][...], 0.0), axis=1, keepdims=True)
    rows = jnp.concatenate([v["mo"][...].astype(F32) * norm, jnp.zeros((96, 2048), F32)], axis=0)
    rows = rows.T.reshape(64, 4, 8, 128)
    packed = rows[:, 0].reshape(512, 128)
    for q in range(1, 4):
        packed = packed + pltpu.roll(rows[:, q].reshape(512, 128), 32 * q, 1)
    msgW[...] = packed.astype(BF16).reshape(64, 8, 128)
    recvW[me] = msgW[me]

    def own_rows(x):
        x = x.reshape(64, 2, 16, x.shape[-1])
        x = jnp.where(first, x[:, 0], x[:, 1])
        return x[:, :8].reshape(512, -1), x[:, 8:].reshape(512, -1)

    def gathered(p, buf, w):
        all_of(rs.at[p], buf)
        x = buf[...].astype(F32)
        squares = jnp.sum(jnp.sum(x * x, axis=0), axis=0, keepdims=True)
        squares = squares + pltpu.roll(squares, 64, 1)
        return dot(w[...], x.reshape(512, 128).astype(BF16)), squares

    def joined(p, own, other, squares, source, target):
        source[0:96] = other
        source[96:104] = jnp.broadcast_to(squares, (8, 128))
        c = swap(p, source, target)
        c.start()
        c.wait()
        squares = squares + target[96:97]
        return (own + target[0:96]) * lax.rsqrt(squares / 2048.0 + EPS)

    u, squares = gathered(0, bufA, wproj)
    u = u[0:224] + pltpu.roll(u[224:448], 64, 1)
    tail = jnp.concatenate(
        [u[128:160], jnp.broadcast_to(squares, (8, 128)), jnp.zeros((24, 128), F32)], axis=0
    )
    by_core = [jnp.concatenate([u[t * 64 : t * 64 + 64], tail], axis=0) for t in range(2)]
    by_seq = jnp.where(low_lanes, by_core[0], pltpu.roll(by_core[1], 64, 1)).T
    msgB[...] = by_seq.reshape(128, 1, 128)
    here_b = tp * N + me
    recvB[here_b] = msgB[here_b]

    def send_parts(i, c):
        t = i
        for core in range(2):
            pltpu.make_async_remote_copy(
                src_ref=msgB.at[core * N + t],
                dst_ref=recvB.at[here_b],
                send_sem=ss.at[1],
                recv_sem=rs.at[1],
                device_id={"kv": t, "tp": core},
                device_id_type=MESH,
            ).start()
        return c

    for t in peers:
        send_parts(t, 0)
    pltpu.make_async_remote_copy(
        src_ref=msgB.at[(1 - tp) * N + me],
        dst_ref=recvB.at[here_b],
        send_sem=ss.at[1],
        recv_sem=rs.at[1],
        device_id={"tp": 1 - tp},
        device_id_type=MESH,
    ).start()
    step_col = jnp.sum(
        jnp.where(iota((64, 128), 1) == me, u[160:224], 0.0), axis=1, keepdims=True
    )
    step_row = jnp.sum(jnp.where(diag, step_col, 0.0), axis=0, keepdims=True)
    sumA[0:1, 0:64] = step_row
    sumA[1:2, :] = squares
    own_swap = swap(0, sumA, pairA)
    own_swap.start()
    send_all(3, lambda t: msgW.at[t], recvW)
    own_swap.wait()
    squares = jnp.where(iota((1, 128), 1) == me, squares + pairA[1:2], 0.0)
    own_rms = lax.rsqrt(jnp.sum(squares, axis=1, keepdims=True) / 2048.0 + EPS)
    step_pre = (own_rms * (step_row + pairA[0:1, 0:64])).astype(BF16).astype(F32)
    shifted = step_pre + v["bias"][...]
    step = jnp.maximum(shifted, 0.0) + jnp.log1p(jnp.exp(-jnp.abs(shifted)))
    decay = -jnp.exp(v["dlog"][...]) * step
    e_total = jnp.exp(decay + cached_row)
    decay_col = jnp.sum(jnp.where(diag, decay, 0.0), axis=1, keepdims=True)
    faded = live * jnp.exp(decay_col + msuf[...])

    n_of, k_of = iota((128, 256), 1), iota((128, 256), 0)
    base = jnp.where(n_of < 128, 80, 64)
    spread = ((k_of - base) == (n_of & 15)).astype(BF16)
    here = ((iota((64, 256), 1) & 127) >> 4) == (iota((64, 256), 0) & 7)
    group = ((iota((64, 64), 0) >> 3) == (iota((64, 64), 1) >> 3)).astype(BF16)
    own_head = iota((64, 32, 64), 0) == iota((64, 32, 64), 2)

    parts = recvB.at[pl.ds(0, 127)]
    pltpu.make_async_copy(parts, parts, rs.at[1]).wait()
    heads = (recvB[0:64] + recvB[64:128]).reshape(64, 128)
    rms = lax.rsqrt(heads[:, 96:97] / 2048.0 + EPS)
    heads = (heads * rms).astype(BF16).astype(F32)
    placed = jnp.where(here, dot(heads.astype(BF16), spread), 0.0).astype(BF16)
    maps = dot(group, placed)
    readout = silu(cio[0] + cio[1] * maps[:, 0:128]).astype(BF16)
    conv_input = silu(cio[2] + cio[3] * maps[:, 128:256])
    readout_f = readout.astype(F32)
    own_score = jnp.sum(readout_f * conv_input, axis=1, keepdims=True)
    own_row = jnp.sum(jnp.where(diag, own_score, 0.0), axis=0, keepdims=True)
    of_group = iota((64, 128), 0) >> 3
    blocks = jnp.concatenate(
        [jnp.where(of_group == g, readout_f, 0.0) for g in range(8)], axis=1
    ).astype(BF16)
    score = dot_t(blocks, v["binput"][...])
    weight = (faded * score).astype(BF16)
    from_block = diagonal(dot_t(v["binner"][...], weight), own_head)
    twice = jnp.concatenate([readout, readout], axis=1)
    from_state = diagonal(dot_t(s2[...], twice), own_head)
    by_channel = heads.T
    conv_inner = silu(cpi[...] + v["tinner"][3] * by_channel[32:64])
    mix = from_block + e_total * from_state + (own_row * step + v["skip"][...]) * conv_inner
    raw = mix * silu(by_channel[0:32])
    by_head = jnp.concatenate([raw, jnp.zeros((96, 64), F32)], axis=0).T
    packed = by_head[0:16]
    for q in range(1, 4):
        packed = packed + pltpu.roll(by_head[q * 16 : (q + 1) * 16], 32 * q, 1)
    srcC[...] = packed.astype(BF16)
    recvC[me] = packed.astype(BF16)
    send_all(2, lambda t: srcC, recvC)

    all_of(rs.at[3], recvW)
    tiles = recvW[...].astype(F32).reshape(4, 128, 128)
    block = iota((128, 128), 1) >> 5
    for dd in range(4):
        out = jnp.zeros((128, 128), F32)
        for q in range(4):
            turned = tiles[q] if q == dd else pltpu.roll(tiles[q], (32 * (q - dd)) % 128, 1)
            out = jnp.where(block == q, turned, out)
        out = out.astype(BF16).reshape(16, 8, 128)
        for i in range(16):
            wd[i // 2, dd * 8 : dd * 8 + 8, (i % 2) * 128 : (i % 2) * 128 + 128] = out[i]

    all_of(rs.at[2], recvC)
    gates = recvC[...].astype(F32)
    gf[...] = gates.reshape(1024, 128)
    partial = jnp.zeros((32, 64), F32)
    for i in range(8):
        pair = [gf[pl.ds(2 * i + e, 64, stride=16), :] for e in range(2)]
        partial = partial + dot_t(wd[i], jnp.concatenate(pair, axis=1).astype(BF16))
    squares = jnp.sum(jnp.sum(gates * gates, axis=1), axis=1, keepdims=True)
    squares = jnp.sum(jnp.where(diag, squares, 0.0), axis=0, keepdims=True)
    squares = jnp.broadcast_to(jnp.concatenate([squares, squares], axis=1), (8, 128))
    part0, part1 = halves(partial[0:16]), halves(partial[16:32])
    sumC[0:8] = jnp.where(first, part1, part0)
    sumC[8:16] = squares
    c = swap(2, sumC, pairC)
    c.start()
    c.wait()
    mixed = jnp.where(first, part0, part1) + pairC[0:8]
    mixed = mixed * lax.rsqrt((squares + pairC[8:16]) / 4096.0 + EPS)
    mid = (x_own + mixed).astype(BF16)
    srcE[...] = mid
    bufE[me] = mid
    send_all(4, lambda t: srcE, bufE)
    for c in mine[2:]:
        c.wait()
    for c in swaps[2:]:
        c.wait()
    gain2 = v["cg"][...]
    we[...] = jnp.zeros((192, 2048), BF16)
    rpt[...] = jnp.zeros((128, 2048), F32)
    for t in range(2):
        we[t * 48 : t * 48 + 44] = (egF[t].astype(F32) * gain2).astype(BF16)
        we[96 + t * 48 : 96 + t * 48 + 44] = (evF[t].astype(F32) * gain2).astype(BF16)
        rpt[t * 48 : t * 48 + 44] = rpF[t].astype(F32)
    pick(we, we2)
    low, up = own_rows(rpt[...].T)
    rt[:, 0:128] = low.astype(BF16)
    rt[:, 128:256] = up.astype(BF16)
    u, squares = gathered(4, bufE, we2)
    own = jnp.where(
        low_lanes,
        u[0:96] + pltpu.roll(u[192:288], 64, 1),
        pltpu.roll(u[96:192], 64, 1) + u[288:384],
    )
    u = joined(4, own, own, squares, sumE, pairE)
    turned = pltpu.roll(u, 64, 1)
    act = silu(jnp.where(low_lanes, u, turned)) * jnp.where(low_lanes, turned, u)
    pad = jnp.zeros((32, 128), F32)
    aa = jnp.concatenate(
        [jnp.where(low_lanes, act, 0.0), pad, jnp.where(low_lanes, 0.0, act), pad], axis=0
    ).astype(BF16)
    msgF[...] = dot(rt[...], aa).astype(BF16).reshape(64, 8, 128)
    recvF[me] = msgF[me]
    send_all(5, lambda t: msgF.at[t], recvF)
    all_of(rs.at[5], recvF)
    end = mid.astype(F32) + jnp.sum(recvF[...].astype(F32), axis=0)
    out_ref[...] = jnp.concatenate([end[:, 0:64], end[:, 64:128]], axis=0)
    for p, b in ((0, bufA), (2, recvC), (3, recvW), (4, bufE), (5, recvF)):
        all_of(ss.at[p], b)
    pltpu.make_async_copy(parts, parts, ss.at[1]).wait()


def shards(
    hidden, mixer_gain, gate_proj, inner_proj, input_proj, output_proj, step_proj, step_bias,
    decay_log, skip_gain, taps_inner, taps_input, taps_output, recent_inner, recent_input,
    recent_output, states, block_inner, block_input, block_decay, lengths, norm_gain, mixer_out,
    channel_gain, expand_gate, expand_value, reduce_proj,
):
    args = dict(
        hid=hidden,
        mg=mixer_gain.reshape(1, 2048),
        gate=gate_proj.transpose(1, 2, 0).reshape(32, 2048),
        inner=inner_proj.transpose(1, 2, 0).reshape(32, 2048),
        inp=input_proj.T,
        outp=output_proj.T,
        stepw=step_proj.T,
        bias=step_bias.reshape(1, 64),
        dlog=decay_log.reshape(1, 64),
        skip=skip_gain.reshape(1, 64),
        tinner=taps_inner.transpose(0, 2, 1),
        tin=taps_input,
        tout=taps_output,
        rinner=recent_inner.transpose(0, 1, 3, 2).reshape(3, 32, 64),
        rin=recent_input.reshape(3, 1024),
        rout=recent_output.reshape(3, 1024),
        states=states.reshape(2048, 128),
        binner=block_inner.transpose(0, 2, 3, 1).reshape(2048, 128),
        binput=block_input.reshape(128, 1024),
        bdecay=block_decay.transpose(0, 2, 1).reshape(64, 128),
        lens=lengths.reshape(1, 1),
        normg=norm_gain.T,
        mo=mixer_out.reshape(32, 2048),
        cg=channel_gain.reshape(1, 2048),
        eg=expand_gate.T,
        ev=expand_value.T,
        rp=reduce_proj,
    )
    away = ("gate", "inner", "eg", "ev", "rp")
    near = [
        pltpu.VMEM(a.shape, a.dtype)
        for n, a in args.items()
        if n not in away
    ]
    scratch = near + [
        pltpu.VMEM((224, 2048), BF16),
        pltpu.VMEM((448, 512), BF16),
        pltpu.VMEM((2, 64, 2048), BF16),
        pltpu.VMEM((2, 44, 2048), BF16),
        pltpu.VMEM((2, 44, 2048), BF16),
        pltpu.VMEM((2, 44, 2048), BF16),
        pltpu.VMEM((192, 2048), BF16),
        pltpu.VMEM((384, 512), BF16),
        pltpu.VMEM((8, 32, 256), BF16),
        pltpu.VMEM((512, 256), BF16),
        pltpu.VMEM((128, 2048), F32),
        pltpu.VMEM((4, 64, 128), F32),
        pltpu.VMEM((32, 64), F32),
        pltpu.VMEM((64, 128), F32),
        pltpu.VMEM((2048, 256), BF16),
        pltpu.VMEM((1024, 128), F32),
        pltpu.VMEM((8, 128), BF16),
        pltpu.VMEM((N, 8, 128), BF16),
        pltpu.VMEM((2 * N, 1, 128), F32),
        pltpu.VMEM((2 * N, 1, 128), F32),
        pltpu.VMEM((8, 128), F32),
        pltpu.VMEM((8, 128), F32),
        pltpu.VMEM((104, 128), F32),
        pltpu.VMEM((104, 128), F32),
        pltpu.VMEM((16, 128), BF16),
        pltpu.VMEM((N, 16, 128), BF16),
        pltpu.VMEM((16, 128), F32),
        pltpu.VMEM((16, 128), F32),
        pltpu.VMEM((N, 8, 128), BF16),
        pltpu.VMEM((N, 8, 128), BF16),
        pltpu.VMEM((8, 128), BF16),
        pltpu.VMEM((N, 8, 128), BF16),
        pltpu.VMEM((N, 8, 128), BF16),
        pltpu.VMEM((N, 8, 128), BF16),
        pltpu.SemaphoreType.DMA((len(near),)),
        pltpu.SemaphoreType.DMA((5,)),
        pltpu.SemaphoreType.DMA((5,)),
        pltpu.SemaphoreType.DMA((5,)),
        pltpu.SemaphoreType.DMA((6,)),
        pltpu.SemaphoreType.DMA((6,)),
        pltpu.SemaphoreType.DMA((6,)),
        pltpu.SemaphoreType.DMA((6,)),
    ]
    space = [
        pl.BlockSpec(memory_space=pltpu.HBM if n == "lens" else pl.ANY) for n in args
    ]
    end = pl.pallas_call(
        kernel,
        out_shape=pltpu.VMEM((16, 64), F32),
        in_specs=space,
        out_specs=pl.BlockSpec(memory_space=pltpu.VMEM),
        scratch_shapes=scratch,
        compiler_params=pltpu.CompilerParams(collective_id=0, has_side_effects=True),
    )(*args.values())
    return end.astype(BF16)


def solution(mesh):
    in_specs = (
        P(KV_TP, "dp"),
        P(),
        P(None, "kv", "tp"),
        P(None, "kv", "tp"),
        P(None, "kv"),
        P(None, "kv"),
        P(),
        P(),
        P(),
        P(),
        P(None, None, "tp"),
        P(),
        P(),
        P(DP_KV, None, None, "tp"),
        P(DP_KV, None, None),
        P(DP_KV, None, None),
        P(DP_KV, None, "tp", None),
        P(DP_KV, None, None, "tp"),
        P(DP_KV, None, None),
        P(DP_KV, None, None),
        P(DP_KV),
        P(None, "tp"),
        P("kv", "tp", None),
        P(),
        P(None, KV_TP),
        P(None, KV_TP),
        P(KV_TP, None),
    )
    return jax.shard_map(
        shards, mesh=mesh, in_specs=in_specs, out_specs=P(KV_TP, "dp"), check_vma=False
    )
```

```python
import jax
import jax.numpy as jnp
from jax import lax
from jax.experimental import pallas as pl
from jax.experimental.pallas import tpu as pltpu
from jax.sharding import PartitionSpec as P

F32 = jnp.float32
BF16 = jnp.bfloat16
MESH = pl.DeviceIdType.MESH
EPS = 1e-05
N = 64
DP_KV = ("dp", "kv")
KV_TP = ("kv", "tp")
NAMES = (
    "hid",
    "mg",
    "gate",
    "inner",
    "inp",
    "outp",
    "stepw",
    "bias",
    "dlog",
    "skip",
    "tinner",
    "tin",
    "tout",
    "rinner",
    "rin",
    "rout",
    "states",
    "binner",
    "binput",
    "bdecay",
    "lens",
    "normg",
    "mo",
    "cg",
    "eg",
    "ev",
    "rp",
)


def silu(v):
    return v / (1.0 + jnp.exp(-v))


def iota(shape, dim):
    return lax.broadcasted_iota(jnp.int32, shape, dim)


def dot(a, b):
    return jnp.dot(a, b, preferred_element_type=F32)


def dot_t(a, b):
    return lax.dot_general(a, b, (((1,), (1,)), ((), ())), preferred_element_type=F32)


def halves(x):
    return jnp.concatenate([x[:8, :], x[8:, :]], axis=1)


def diagonal(d, mask):
    return jnp.sum(jnp.where(mask, d.reshape(64, 32, 64), 0.0), axis=0)


def kernel(*refs):
    names = NAMES
    h = dict(zip(names, refs))
    out_ref = refs[len(names)]
    local = [n for n in names if n not in ("gate", "inner", "eg", "ev", "rp")]
    rest = refs[len(names) + 1 :]
    v = dict(zip(local, rest))
    (
        wfull, wproj, giF, egF, evF, rpF, we, we2, wd, rt, rpt, cio, cpi, msuf, s2, gf,
        srcA, bufA, msgB, recvB, sumA, pairA, otherA, sumF, pairF, srcC, recvC, sumC, pairC, msgW, recvW, srcE, bufE, msgF, recvF,
        lsem, csem, xs, xr, ss, rs, ps, pr,
    ) = rest[len(local) :]
    me, tp = lax.axis_index("kv"), lax.axis_index("tp")
    first = tp == 0

    order = (4, 3, 5, 2, 6, 1, 7, 0)
    in_rows = [lax.rem(me // 8 + o, 8) * 8 for o in order]
    in_cols = [lax.rem(lax.rem(me, 8) + o, 8) for o in order]
    peers = [r + c for r in in_rows for c in in_cols][: N - 1]
    dist = [min(o, 8 - o) for o in order]
    ranks = sorted(range(N - 1), key=lambda i: -(dist[i // 8] + dist[i % 8]))
    peers = [peers[i] for i in ranks]

    barrier = pltpu.get_barrier_semaphore()

    pl.semaphore_signal(barrier, inc=1, device_id={"tp": 1 - tp}, device_id_type=MESH)
    for t in peers:
        pl.semaphore_signal(barrier, inc=1, device_id={"kv": t}, device_id_type=MESH)

    loads = {n: pltpu.make_async_copy(h[n], v[n], lsem.at[i]) for i, n in enumerate(local)}
    shared = (
        ("gate", giF.at[tp, pl.ds(0, 32)]),
        ("inner", giF.at[tp, pl.ds(32, 32)]),
        ("eg", egF.at[tp]),
        ("ev", evF.at[tp]),
        ("rp", rpF.at[tp]),
    )
    mine = [pltpu.make_async_copy(h[n], f, csem.at[i]) for i, (n, f) in enumerate(shared)]
    for c in loads.values():
        c.start()
    for c in mine:
        c.start()

    def send_all(p, source, target):
        def one(i, c):
            t = i
            pltpu.make_async_remote_copy(
                src_ref=source(t),
                dst_ref=target.at[me],
                send_sem=ss.at[p],
                recv_sem=rs.at[p],
                device_id={"kv": t},
                device_id_type=MESH,
            ).start()
            return c

        for t in peers:
            one(t, 0)

    def all_of(sem, buf):
        most = buf.at[pl.ds(0, N - 1)]
        pltpu.make_async_copy(most, most, sem).wait()

    def swap(p, source, target):
        return pltpu.make_async_remote_copy(
            src_ref=source,
            dst_ref=target,
            send_sem=ps.at[p],
            recv_sem=pr.at[p],
            device_id={"tp": 1 - tp},
            device_id_type=MESH,
        )

    loads["hid"].wait()
    x_own = halves(v["hid"][...].astype(F32))
    srcA[...] = x_own.astype(BF16)
    bufA[me] = x_own.astype(BF16)
    pl.semaphore_wait(barrier, N)

    send_all(0, lambda t: srcA, bufA)
    hid_swap = swap(5, srcA, otherA)
    hid_swap.start()
    swaps = [
        pltpu.make_async_remote_copy(
            src_ref=h[n],
            dst_ref=f,
            send_sem=xs.at[i],
            recv_sem=xr.at[i],
            device_id={"tp": 1 - tp},
            device_id_type=MESH,
        )
        for i, (n, f) in enumerate(shared)
    ]
    for c in swaps:
        c.start()
    for n in local:
        if n != "hid":
            loads[n].wait()

    gain = v["mg"][...]
    wfull[128:144] = (v["inp"][...].astype(F32) * gain).astype(BF16)
    wfull[144:160] = (v["outp"][...].astype(F32) * gain).astype(BF16)
    wfull[160:224] = (v["stepw"][...].astype(F32) * gain).astype(BF16)
    low_lanes = iota((1, 128), 1) < 64
    to, at = iota((512, 256), 0), iota((512, 256), 1)
    spot = ((at & 127) >> 3) * 32 + (at >> 7) * 8 + (at & 7)

    def picked_of(t):
        return (to == spot + 16 * t).astype(BF16)

    def pick(whole, out, picked):
        n = whole.shape[0]
        for i in range(4):
            y = dot(whole[:, i * 512 : (i + 1) * 512], picked).astype(BF16)
            out[0:n, i * 128 : (i + 1) * 128] = y[:, 0:128]
            out[n : 2 * n, i * 128 : (i + 1) * 128] = y[:, 128:256]

    for c in mine[:2]:
        c.wait()
    for c in swaps[:2]:
        c.wait()
    for t in range(2):
        wfull[t * 64 : t * 64 + 64] = (giF[t].astype(F32) * gain).astype(BF16)
    pick(wfull, wproj, picked_of(tp))

    for a, (t, r) in enumerate((("tout", "rout"), ("tin", "rin"))):
        taps, rec = v[t][...], v[r][...].astype(F32)
        past = jnp.sum(rec * taps[:3], axis=0, keepdims=True)
        for g in range(8):
            at = slice(g * 128, (g + 1) * 128)
            cio[2 * a, g * 8 : (g + 1) * 8] = jnp.broadcast_to(past[:, at], (8, 128))
            cio[2 * a + 1, g * 8 : (g + 1) * 8] = jnp.broadcast_to(taps[3:4, at], (8, 128))
    taps, rec = v["tinner"], v["rinner"]
    cpi[...] = (
        taps[0] * rec[0].astype(F32) + taps[1] * rec[1].astype(F32) + taps[2] * rec[2].astype(F32)
    )

    live = (iota((64, 128), 1) < v["lens"][0:1, 0:1]).astype(F32)
    masked = v["bdecay"][...] * live
    later = (iota((128, 128), 0) > iota((128, 128), 1)).astype(F32)
    msuf[...] = jnp.dot(
        masked, later, preferred_element_type=F32, precision=lax.Precision.HIGHEST
    )
    diag = iota((64, 64), 0) == iota((64, 64), 1)
    cached = jnp.sum(masked, axis=1, keepdims=True)
    cached_row = jnp.sum(jnp.where(diag, cached, 0.0), axis=0, keepdims=True)
    whole = v["states"][...]
    high = whole.astype(BF16)
    s2[:, 0:128] = high
    s2[:, 128:256] = (whole - high.astype(F32)).astype(BF16)

    lane = iota((32, 64), 1)
    norm = jnp.sum(jnp.where(lane == me, v["normg"][...], 0.0), axis=1, keepdims=True)
    rows = jnp.concatenate([v["mo"][...].astype(F32) * norm, jnp.zeros((96, 2048), F32)], axis=0)
    rows = rows.T.reshape(64, 4, 8, 128)
    packed = rows[:, 0].reshape(512, 128)
    for q in range(1, 4):
        packed = packed + pltpu.roll(rows[:, q].reshape(512, 128), 32 * q, 1)
    msgW[...] = packed.astype(BF16).reshape(64, 8, 128)
    recvW[me] = msgW[me]

    def gathered(p, buf, w):
        all_of(rs.at[p], buf)
        x = buf[...].astype(F32)
        squares = jnp.sum(jnp.sum(x * x, axis=0), axis=0, keepdims=True)
        squares = squares + pltpu.roll(squares, 64, 1)
        return dot(w[...], x.reshape(512, 128).astype(BF16)), squares

    u, squares = gathered(0, bufA, wproj)
    u = u[0:224] + pltpu.roll(u[224:448], 64, 1)
    tail = jnp.concatenate(
        [u[128:160], jnp.broadcast_to(squares, (8, 128)), jnp.zeros((24, 128), F32)], axis=0
    )
    by_core = [jnp.concatenate([u[t * 64 : t * 64 + 64], tail], axis=0) for t in range(2)]
    by_seq = jnp.where(low_lanes, by_core[0], pltpu.roll(by_core[1], 64, 1)).T
    msgB[...] = by_seq.reshape(128, 1, 128)
    here_b = tp * N + me
    recvB[here_b] = msgB[here_b]

    def send_parts(i, c):
        t = i
        for core in range(2):
            pltpu.make_async_remote_copy(
                src_ref=msgB.at[core * N + t],
                dst_ref=recvB.at[here_b],
                send_sem=ss.at[1],
                recv_sem=rs.at[1],
                device_id={"kv": t, "tp": core},
                device_id_type=MESH,
            ).start()
        return c

    for t in peers:
        send_parts(t, 0)
    pltpu.make_async_remote_copy(
        src_ref=msgB.at[(1 - tp) * N + me],
        dst_ref=recvB.at[here_b],
        send_sem=ss.at[1],
        recv_sem=rs.at[1],
        device_id={"tp": 1 - tp},
        device_id_type=MESH,
    ).start()
    step_col = jnp.sum(
        jnp.where(iota((64, 128), 1) == me, u[160:224], 0.0), axis=1, keepdims=True
    )
    step_row = jnp.sum(jnp.where(diag, step_col, 0.0), axis=0, keepdims=True)
    sumA[0:1, 0:64] = step_row
    sumA[1:2, :] = squares
    own_swap = swap(0, sumA, pairA)
    own_swap.start()
    send_all(3, lambda t: msgW.at[t], recvW)
    own_swap.wait()
    squares = jnp.where(iota((1, 128), 1) == me, squares + pairA[1:2], 0.0)
    own_rms = lax.rsqrt(jnp.sum(squares, axis=1, keepdims=True) / 2048.0 + EPS)
    step_pre = (own_rms * (step_row + pairA[0:1, 0:64])).astype(BF16).astype(F32)
    shifted = step_pre + v["bias"][...]
    step = jnp.maximum(shifted, 0.0) + jnp.log1p(jnp.exp(-jnp.abs(shifted)))
    decay = -jnp.exp(v["dlog"][...]) * step
    e_total = jnp.exp(decay + cached_row)
    decay_col = jnp.sum(jnp.where(diag, decay, 0.0), axis=1, keepdims=True)
    faded = live * jnp.exp(decay_col + msuf[...])

    n_of, k_of = iota((128, 256), 1), iota((128, 256), 0)
    base = jnp.where(n_of < 128, 80, 64)
    spread = ((k_of - base) == (n_of & 15)).astype(BF16)
    here = ((iota((64, 256), 1) & 127) >> 4) == (iota((64, 256), 0) & 7)
    group = ((iota((64, 64), 0) >> 3) == (iota((64, 64), 1) >> 3)).astype(BF16)
    own_head = iota((64, 32, 64), 0) == iota((64, 32, 64), 2)

    parts = recvB.at[pl.ds(0, 127)]
    pltpu.make_async_copy(parts, parts, rs.at[1]).wait()
    heads = (recvB[0:64] + recvB[64:128]).reshape(64, 128)
    rms = lax.rsqrt(heads[:, 96:97] / 2048.0 + EPS)
    heads = (heads * rms).astype(BF16).astype(F32)
    placed = jnp.where(here, dot(heads.astype(BF16), spread), 0.0).astype(BF16)
    maps = dot(group, placed)
    readout = silu(cio[0] + cio[1] * maps[:, 0:128]).astype(BF16)
    conv_input = silu(cio[2] + cio[3] * maps[:, 128:256])
    readout_f = readout.astype(F32)
    own_score = jnp.sum(readout_f * conv_input, axis=1, keepdims=True)
    own_row = jnp.sum(jnp.where(diag, own_score, 0.0), axis=0, keepdims=True)
    of_group = iota((64, 128), 0) >> 3
    blocks = jnp.concatenate(
        [jnp.where(of_group == g, readout_f, 0.0) for g in range(8)], axis=1
    ).astype(BF16)
    score = dot_t(blocks, v["binput"][...])
    weight = (faded * score).astype(BF16)
    from_block = diagonal(dot_t(v["binner"][...], weight), own_head)
    twice = jnp.concatenate([readout, readout], axis=1)
    from_state = diagonal(dot_t(s2[...], twice), own_head)
    by_channel = heads.T
    conv_inner = silu(cpi[...] + v["tinner"][3] * by_channel[32:64])
    mix = from_block + e_total * from_state + (own_row * step + v["skip"][...]) * conv_inner
    raw = mix * silu(by_channel[0:32])
    by_head = jnp.concatenate([raw, jnp.zeros((96, 64), F32)], axis=0).T
    packed = by_head[0:16]
    for q in range(1, 4):
        packed = packed + pltpu.roll(by_head[q * 16 : (q + 1) * 16], 32 * q, 1)
    srcC[...] = packed.astype(BF16)
    recvC[me] = packed.astype(BF16)
    send_all(2, lambda t: srcC, recvC)

    all_of(rs.at[3], recvW)
    tiles = recvW[...].astype(F32).reshape(4, 128, 128)
    block = iota((128, 128), 1) >> 5
    for dd in range(4):
        out = jnp.zeros((128, 128), F32)
        for q in range(4):
            turned = tiles[q] if q == dd else pltpu.roll(tiles[q], (32 * (q - dd)) % 128, 1)
            out = jnp.where(block == q, turned, out)
        out = out.astype(BF16).reshape(16, 8, 128)
        for i in range(16):
            wd[i // 2, dd * 8 : dd * 8 + 8, (i % 2) * 128 : (i % 2) * 128 + 128] = out[i]

    all_of(rs.at[2], recvC)
    gates = recvC[...].astype(F32)
    gf[...] = gates.reshape(1024, 128)
    partial = jnp.zeros((32, 64), F32)
    for i in range(8):
        pair = [gf[pl.ds(2 * i + e, 64, stride=16), :] for e in range(2)]
        partial = partial + dot_t(wd[i], jnp.concatenate(pair, axis=1).astype(BF16))
    squares = jnp.sum(jnp.sum(gates * gates, axis=1), axis=1, keepdims=True)
    squares = jnp.sum(jnp.where(diag, squares, 0.0), axis=0, keepdims=True)
    squares = jnp.broadcast_to(jnp.concatenate([squares, squares], axis=1), (8, 128))
    part0, part1 = halves(partial[0:16]), halves(partial[16:32])
    hid_swap.wait()
    for c in swaps[2:]:
        c.wait_recv()

    def unpacked(x):
        return jnp.concatenate([x[:, 0:64], x[:, 64:128]], axis=0)

    @pl.when(tp == 0)
    def _():
        sumC[0:8] = part0
        sumC[8:16] = part1
        sumC[16:24] = squares
        c = swap(2, sumC, pairC)
        c.start()
        c.wait_send()
        pltpu.make_async_copy(pairF, pairF, pr.at[4]).wait()
        out_ref[...] = unpacked(pairF[...])

    @pl.when(tp == 1)
    def _():
        pltpu.make_async_copy(pairC, pairC, pr.at[2]).wait()
        scale = lax.rsqrt((squares + pairC[16:24]) / 4096.0 + EPS)
        mids = []
        for t, (x, part) in enumerate(((otherA[...].astype(F32), part0), (x_own, part1))):
            mids.append((x + (part + pairC[t * 8 : t * 8 + 8]) * scale).astype(BF16))
            srcE[t] = mids[t]
            bufE[me, t] = mids[t]
        send_all(4, lambda t: srcE, bufE)
        for c in mine[2:]:
            c.wait()
        gain2 = v["cg"][...]
        we[...] = jnp.zeros((192, 2048), BF16)
        rpt[...] = jnp.zeros((128, 2048), F32)
        for t in range(2):
            we[t * 48 : t * 48 + 44] = (egF[t].astype(F32) * gain2).astype(BF16)
            we[96 + t * 48 : 96 + t * 48 + 44] = (evF[t].astype(F32) * gain2).astype(BF16)
            rpt[t * 48 : t * 48 + 44] = rpF[t].astype(F32)
        by_row = rpt[...].T.reshape(64, 4, 8, 128)
        for t in range(2):
            pick(we, we2.at[t], picked_of(t))
            for b in range(2):
                part = by_row[:, 2 * t + b].reshape(512, 128)
                rt[t, :, b * 128 : (b + 1) * 128] = part.astype(BF16)
        all_of(rs.at[4], bufE)
        y = bufE[...].astype(F32)
        squares2 = jnp.sum(jnp.sum(y * y, axis=(0, 1)), axis=0, keepdims=True)
        squares2 = squares2 + pltpu.roll(squares2, 64, 1)
        u = dot(we2[0], y[:, 0].reshape(512, 128).astype(BF16))
        u = u + dot(we2[1], y[:, 1].reshape(512, 128).astype(BF16))
        u = jnp.where(
            low_lanes,
            u[0:96] + pltpu.roll(u[192:288], 64, 1),
            pltpu.roll(u[96:192], 64, 1) + u[288:384],
        )
        u = u * lax.rsqrt(squares2 / 2048.0 + EPS)
        turned = pltpu.roll(u, 64, 1)
        act = silu(jnp.where(low_lanes, u, turned)) * jnp.where(low_lanes, turned, u)
        pad = jnp.zeros((32, 128), F32)
        aa = jnp.concatenate(
            [jnp.where(low_lanes, act, 0.0), pad, jnp.where(low_lanes, 0.0, act), pad], axis=0
        ).astype(BF16)
        for t in range(2):
            msgF[:, t] = dot(rt[t], aa).astype(BF16).reshape(64, 8, 128)
        recvF[me] = msgF[me]
        send_all(5, lambda t: msgF.at[t], recvF)
        all_of(rs.at[5], recvF)
        tot = jnp.sum(recvF[...].astype(F32), axis=0)
        sumF[...] = mids[0].astype(F32) + tot[0]
        c = swap(4, sumF, pairF)
        c.start()
        out_ref[...] = unpacked(mids[1].astype(F32) + tot[1])
        c.wait_send()
        all_of(ss.at[4], bufE)
        all_of(ss.at[5], recvF)

    @pl.when(tp == 0)
    def _():
        for c in mine[2:]:
            c.wait()

    for c in swaps[2:]:
        c.wait_send()
    for p, b in ((0, bufA), (2, recvC), (3, recvW)):
        all_of(ss.at[p], b)
    pltpu.make_async_copy(parts, parts, ss.at[1]).wait()


def shards(
    hidden, mixer_gain, gate_proj, inner_proj, input_proj, output_proj, step_proj, step_bias,
    decay_log, skip_gain, taps_inner, taps_input, taps_output, recent_inner, recent_input,
    recent_output, states, block_inner, block_input, block_decay, lengths, norm_gain, mixer_out,
    channel_gain, expand_gate, expand_value, reduce_proj,
):
    args = dict(
        hid=hidden,
        mg=mixer_gain.reshape(1, 2048),
        gate=gate_proj.transpose(1, 2, 0).reshape(32, 2048),
        inner=inner_proj.transpose(1, 2, 0).reshape(32, 2048),
        inp=input_proj.T,
        outp=output_proj.T,
        stepw=step_proj.T,
        bias=step_bias.reshape(1, 64),
        dlog=decay_log.reshape(1, 64),
        skip=skip_gain.reshape(1, 64),
        tinner=taps_inner.transpose(0, 2, 1),
        tin=taps_input,
        tout=taps_output,
        rinner=recent_inner.transpose(0, 1, 3, 2).reshape(3, 32, 64),
        rin=recent_input.reshape(3, 1024),
        rout=recent_output.reshape(3, 1024),
        states=states.reshape(2048, 128),
        binner=block_inner.transpose(0, 2, 3, 1).reshape(2048, 128),
        binput=block_input.reshape(128, 1024),
        bdecay=block_decay.transpose(0, 2, 1).reshape(64, 128),
        lens=lengths.reshape(1, 1),
        normg=norm_gain.T,
        mo=mixer_out.reshape(32, 2048),
        cg=channel_gain.reshape(1, 2048),
        eg=expand_gate.T,
        ev=expand_value.T,
        rp=reduce_proj,
    )
    away = ("gate", "inner", "eg", "ev", "rp")
    near = [
        pltpu.VMEM(a.shape, a.dtype)
        for n, a in args.items()
        if n not in away
    ]
    scratch = near + [
        pltpu.VMEM((224, 2048), BF16),
        pltpu.VMEM((448, 512), BF16),
        pltpu.VMEM((2, 64, 2048), BF16),
        pltpu.VMEM((2, 44, 2048), BF16),
        pltpu.VMEM((2, 44, 2048), BF16),
        pltpu.VMEM((2, 44, 2048), BF16),
        pltpu.VMEM((192, 2048), BF16),
        pltpu.VMEM((2, 384, 512), BF16),
        pltpu.VMEM((8, 32, 256), BF16),
        pltpu.VMEM((2, 512, 256), BF16),
        pltpu.VMEM((128, 2048), F32),
        pltpu.VMEM((4, 64, 128), F32),
        pltpu.VMEM((32, 64), F32),
        pltpu.VMEM((64, 128), F32),
        pltpu.VMEM((2048, 256), BF16),
        pltpu.VMEM((1024, 128), F32),
        pltpu.VMEM((8, 128), BF16),
        pltpu.VMEM((N, 8, 128), BF16),
        pltpu.VMEM((2 * N, 1, 128), F32),
        pltpu.VMEM((2 * N, 1, 128), F32),
        pltpu.VMEM((8, 128), F32),
        pltpu.VMEM((8, 128), F32),
        pltpu.VMEM((8, 128), BF16),
        pltpu.VMEM((8, 128), F32),
        pltpu.VMEM((8, 128), F32),
        pltpu.VMEM((16, 128), BF16),
        pltpu.VMEM((N, 16, 128), BF16),
        pltpu.VMEM((24, 128), F32),
        pltpu.VMEM((24, 128), F32),
        pltpu.VMEM((N, 8, 128), BF16),
        pltpu.VMEM((N, 8, 128), BF16),
        pltpu.VMEM((2, 8, 128), BF16),
        pltpu.VMEM((N, 2, 8, 128), BF16),
        pltpu.VMEM((N, 2, 8, 128), BF16),
        pltpu.VMEM((N, 2, 8, 128), BF16),
        pltpu.SemaphoreType.DMA((len(near),)),
        pltpu.SemaphoreType.DMA((5,)),
        pltpu.SemaphoreType.DMA((5,)),
        pltpu.SemaphoreType.DMA((5,)),
        pltpu.SemaphoreType.DMA((6,)),
        pltpu.SemaphoreType.DMA((6,)),
        pltpu.SemaphoreType.DMA((6,)),
        pltpu.SemaphoreType.DMA((6,)),
    ]
    space = [
        pl.BlockSpec(memory_space=pltpu.HBM if n == "lens" else pl.ANY) for n in args
    ]
    end = pl.pallas_call(
        kernel,
        out_shape=pltpu.VMEM((16, 64), F32),
        in_specs=space,
        out_specs=pl.BlockSpec(memory_space=pltpu.VMEM),
        scratch_shapes=scratch,
        compiler_params=pltpu.CompilerParams(collective_id=0, has_side_effects=True),
    )(*args.values())
    return end.astype(BF16)


def solution(mesh):
    in_specs = (
        P(KV_TP, "dp"),
        P(),
        P(None, "kv", "tp"),
        P(None, "kv", "tp"),
        P(None, "kv"),
        P(None, "kv"),
        P(),
        P(),
        P(),
        P(),
        P(None, None, "tp"),
        P(),
        P(),
        P(DP_KV, None, None, "tp"),
        P(DP_KV, None, None),
        P(DP_KV, None, None),
        P(DP_KV, None, "tp", None),
        P(DP_KV, None, None, "tp"),
        P(DP_KV, None, None),
        P(DP_KV, None, None),
        P(DP_KV),
        P(None, "tp"),
        P("kv", "tp", None),
        P(),
        P(None, KV_TP),
        P(None, KV_TP),
        P(KV_TP, None),
    )
    return jax.shard_map(
        shards, mesh=mesh, in_specs=in_specs, out_specs=P(KV_TP, "dp"), check_vma=False
    )
```

```python
import jax
import jax.numpy as jnp
from jax import lax
from jax.experimental import pallas as pl
from jax.experimental.pallas import tpu as pltpu
from jax.sharding import PartitionSpec as P

F32 = jnp.float32
BF16 = jnp.bfloat16
MESH = pl.DeviceIdType.MESH
EPS = 1e-05
N = 64
DP_KV = ("dp", "kv")
KV_TP = ("kv", "tp")
NAMES = (
    "hid",
    "mg",
    "gate",
    "inner",
    "inp",
    "outp",
    "stepw",
    "bias",
    "dlog",
    "skip",
    "tinner",
    "tin",
    "tout",
    "rinner",
    "rin",
    "rout",
    "states",
    "binner",
    "binput",
    "bdecay",
    "lens",
    "normg",
    "mo",
    "cg",
    "eg",
    "ev",
    "rp",
)


def silu(v):
    return v / (1.0 + jnp.exp(-v))


def iota(shape, dim):
    return lax.broadcasted_iota(jnp.int32, shape, dim)


def dot(a, b):
    return jnp.dot(a, b, preferred_element_type=F32)


def dot_t(a, b):
    return lax.dot_general(a, b, (((1,), (1,)), ((), ())), preferred_element_type=F32)


def halves(x):
    return jnp.concatenate([x[:8, :], x[8:, :]], axis=1)


def diagonal(d, mask):
    return jnp.sum(jnp.where(mask, d.reshape(64, 32, 64), 0.0), axis=0)


def kernel(*refs):
    names = NAMES
    h = dict(zip(names, refs))
    out_ref = refs[len(names)]
    local = [n for n in names if n not in ("gate", "inner", "eg", "ev", "rp")]
    rest = refs[len(names) + 1 :]
    v = dict(zip(local, rest))
    (
        wfull, wproj, giF, egF, evF, rpF, we, we2, wd, rt, rpt, cio, cpi, msuf, s2, gf,
        srcA, bufA, msgB, recvB, sumA, pairA, otherA, sumF, pairF, srcC, recvC, msgW, recvW, srcE, bufE, msgF, recvF,
        lsem, csem, xs, xr, ss, rs, ps, pr,
    ) = rest[len(local) :]
    me, tp = lax.axis_index("kv"), lax.axis_index("tp")
    here_b = tp * N + me

    order = (4, 3, 5, 2, 6, 1, 7, 0)
    in_rows = [lax.rem(me // 8 + o, 8) * 8 for o in order]
    in_cols = [lax.rem(lax.rem(me, 8) + o, 8) for o in order]
    peers = [r + c for r in in_rows for c in in_cols][: N - 1]
    dist = [min(o, 8 - o) for o in order]
    ranks = sorted(range(N - 1), key=lambda i: -(dist[i // 8] + dist[i % 8]))
    peers = [peers[i] for i in ranks]

    barrier = pltpu.get_barrier_semaphore()

    pl.semaphore_signal(barrier, inc=1, device_id={"tp": 1 - tp}, device_id_type=MESH)
    for t in peers:
        pl.semaphore_signal(barrier, inc=1, device_id={"kv": t}, device_id_type=MESH)

    loads = {n: pltpu.make_async_copy(h[n], v[n], lsem.at[i]) for i, n in enumerate(local)}
    shared = (
        ("gate", giF.at[tp, pl.ds(0, 32)]),
        ("inner", giF.at[tp, pl.ds(32, 32)]),
        ("eg", egF.at[tp]),
        ("ev", evF.at[tp]),
        ("rp", rpF.at[tp]),
    )
    mine = [pltpu.make_async_copy(h[n], f, csem.at[i]) for i, (n, f) in enumerate(shared)]
    for c in loads.values():
        c.start()
    for c in mine:
        c.start()

    def send_all(p, source, target):
        def one(i, c):
            t = i
            pltpu.make_async_remote_copy(
                src_ref=source(t),
                dst_ref=target.at[me],
                send_sem=ss.at[p],
                recv_sem=rs.at[p],
                device_id={"kv": t},
                device_id_type=MESH,
            ).start()
            return c

        for t in peers:
            one(t, 0)

    def to_last(p, source, target):
        def one(t):
            pltpu.make_async_remote_copy(
                src_ref=source(me if t is None else t),
                dst_ref=target.at[here_b],
                send_sem=ss.at[p],
                recv_sem=rs.at[p],
                device_id={"tp": 1} if t is None else {"kv": t, "tp": 1},
                device_id_type=MESH,
            ).start()

        for t in peers:
            one(t)

        @pl.when(tp == 0)
        def _():
            one(None)

    def count(sem, buf, n):
        some = buf.at[pl.ds(0, n)]
        pltpu.make_async_copy(some, some, sem).wait()

    def all_of(sem, buf):
        most = buf.at[pl.ds(0, N - 1)]
        pltpu.make_async_copy(most, most, sem).wait()

    def swap(p, source, target):
        return pltpu.make_async_remote_copy(
            src_ref=source,
            dst_ref=target,
            send_sem=ps.at[p],
            recv_sem=pr.at[p],
            device_id={"tp": 1 - tp},
            device_id_type=MESH,
        )

    loads["hid"].wait()
    x_own = halves(v["hid"][...].astype(F32))
    srcA[...] = x_own.astype(BF16)
    bufA[me] = x_own.astype(BF16)
    pl.semaphore_wait(barrier, N)

    send_all(0, lambda t: srcA, bufA)
    hid_swap = swap(5, srcA, otherA)
    hid_swap.start()
    swaps = [
        pltpu.make_async_remote_copy(
            src_ref=h[n],
            dst_ref=f,
            send_sem=xs.at[i],
            recv_sem=xr.at[i],
            device_id={"tp": 1 - tp},
            device_id_type=MESH,
        )
        for i, (n, f) in enumerate(shared)
    ]
    for c in swaps:
        c.start()
    for n in local:
        if n != "hid":
            loads[n].wait()

    gain = v["mg"][...]
    wfull[128:144] = (v["inp"][...].astype(F32) * gain).astype(BF16)
    wfull[144:160] = (v["outp"][...].astype(F32) * gain).astype(BF16)
    wfull[160:224] = (v["stepw"][...].astype(F32) * gain).astype(BF16)
    low_lanes = iota((1, 128), 1) < 64
    to, at = iota((512, 256), 0), iota((512, 256), 1)
    spot = ((at & 127) >> 3) * 32 + (at >> 7) * 8 + (at & 7)

    def picked_of(t):
        return (to == spot + 16 * t).astype(BF16)

    def pick(whole, out, picked):
        n = whole.shape[0]
        for i in range(4):
            y = dot(whole[:, i * 512 : (i + 1) * 512], picked).astype(BF16)
            out[0:n, i * 128 : (i + 1) * 128] = y[:, 0:128]
            out[n : 2 * n, i * 128 : (i + 1) * 128] = y[:, 128:256]

    for c in mine[:2]:
        c.wait()
    for c in swaps[:2]:
        c.wait()
    for t in range(2):
        wfull[t * 64 : t * 64 + 64] = (giF[t].astype(F32) * gain).astype(BF16)
    pick(wfull, wproj, picked_of(tp))

    for a, (t, r) in enumerate((("tout", "rout"), ("tin", "rin"))):
        taps, rec = v[t][...], v[r][...].astype(F32)
        past = jnp.sum(rec * taps[:3], axis=0, keepdims=True)
        for g in range(8):
            at = slice(g * 128, (g + 1) * 128)
            cio[2 * a, g * 8 : (g + 1) * 8] = jnp.broadcast_to(past[:, at], (8, 128))
            cio[2 * a + 1, g * 8 : (g + 1) * 8] = jnp.broadcast_to(taps[3:4, at], (8, 128))
    taps, rec = v["tinner"], v["rinner"]
    cpi[...] = (
        taps[0] * rec[0].astype(F32) + taps[1] * rec[1].astype(F32) + taps[2] * rec[2].astype(F32)
    )

    live = (iota((64, 128), 1) < v["lens"][0:1, 0:1]).astype(F32)
    masked = v["bdecay"][...] * live
    later = (iota((128, 128), 0) > iota((128, 128), 1)).astype(F32)
    msuf[...] = jnp.dot(
        masked, later, preferred_element_type=F32, precision=lax.Precision.HIGHEST
    )
    diag = iota((64, 64), 0) == iota((64, 64), 1)
    cached = jnp.sum(masked, axis=1, keepdims=True)
    cached_row = jnp.sum(jnp.where(diag, cached, 0.0), axis=0, keepdims=True)
    whole = v["states"][...]
    high = whole.astype(BF16)
    s2[:, 0:128] = high
    s2[:, 128:256] = (whole - high.astype(F32)).astype(BF16)

    lane = iota((32, 64), 1)
    norm = jnp.sum(jnp.where(lane == me, v["normg"][...], 0.0), axis=1, keepdims=True)
    rows = jnp.concatenate([v["mo"][...].astype(F32) * norm, jnp.zeros((96, 2048), F32)], axis=0)
    rows = rows.T.reshape(64, 4, 8, 128)
    packed = rows[:, 0].reshape(512, 128)
    for q in range(1, 4):
        packed = packed + pltpu.roll(rows[:, q].reshape(512, 128), 32 * q, 1)
    msgW[...] = packed.astype(BF16).reshape(64, 8, 128)
    recvW[here_b] = msgW[me]

    def gathered(p, buf, w):
        all_of(rs.at[p], buf)
        x = buf[...].astype(F32)
        squares = jnp.sum(jnp.sum(x * x, axis=0), axis=0, keepdims=True)
        squares = squares + pltpu.roll(squares, 64, 1)
        return dot(w[...], x.reshape(512, 128).astype(BF16)), squares

    u, squares = gathered(0, bufA, wproj)
    u = u[0:224] + pltpu.roll(u[224:448], 64, 1)
    tail = jnp.concatenate(
        [u[128:160], jnp.broadcast_to(squares, (8, 128)), jnp.zeros((24, 128), F32)], axis=0
    )
    by_core = [jnp.concatenate([u[t * 64 : t * 64 + 64], tail], axis=0) for t in range(2)]
    by_seq = jnp.where(low_lanes, by_core[0], pltpu.roll(by_core[1], 64, 1)).T
    msgB[...] = by_seq.reshape(128, 1, 128)
    recvB[here_b] = msgB[here_b]

    def send_parts(i, c):
        t = i
        for core in range(2):
            pltpu.make_async_remote_copy(
                src_ref=msgB.at[core * N + t],
                dst_ref=recvB.at[here_b],
                send_sem=ss.at[1],
                recv_sem=rs.at[1],
                device_id={"kv": t, "tp": core},
                device_id_type=MESH,
            ).start()
        return c

    for t in peers:
        send_parts(t, 0)
    pltpu.make_async_remote_copy(
        src_ref=msgB.at[(1 - tp) * N + me],
        dst_ref=recvB.at[here_b],
        send_sem=ss.at[1],
        recv_sem=rs.at[1],
        device_id={"tp": 1 - tp},
        device_id_type=MESH,
    ).start()
    step_col = jnp.sum(
        jnp.where(iota((64, 128), 1) == me, u[160:224], 0.0), axis=1, keepdims=True
    )
    step_row = jnp.sum(jnp.where(diag, step_col, 0.0), axis=0, keepdims=True)
    sumA[0:1, 0:64] = step_row
    sumA[1:2, :] = squares
    own_swap = swap(0, sumA, pairA)
    own_swap.start()
    to_last(3, lambda t: msgW.at[t], recvW)
    own_swap.wait()
    squares = jnp.where(iota((1, 128), 1) == me, squares + pairA[1:2], 0.0)
    own_rms = lax.rsqrt(jnp.sum(squares, axis=1, keepdims=True) / 2048.0 + EPS)
    step_pre = (own_rms * (step_row + pairA[0:1, 0:64])).astype(BF16).astype(F32)
    shifted = step_pre + v["bias"][...]
    step = jnp.maximum(shifted, 0.0) + jnp.log1p(jnp.exp(-jnp.abs(shifted)))
    decay = -jnp.exp(v["dlog"][...]) * step
    e_total = jnp.exp(decay + cached_row)
    decay_col = jnp.sum(jnp.where(diag, decay, 0.0), axis=1, keepdims=True)
    faded = live * jnp.exp(decay_col + msuf[...])

    n_of, k_of = iota((128, 256), 1), iota((128, 256), 0)
    base = jnp.where(n_of < 128, 80, 64)
    spread = ((k_of - base) == (n_of & 15)).astype(BF16)
    here = ((iota((64, 256), 1) & 127) >> 4) == (iota((64, 256), 0) & 7)
    group = ((iota((64, 64), 0) >> 3) == (iota((64, 64), 1) >> 3)).astype(BF16)
    own_head = iota((64, 32, 64), 0) == iota((64, 32, 64), 2)

    parts = recvB.at[pl.ds(0, 127)]
    pltpu.make_async_copy(parts, parts, rs.at[1]).wait()
    heads = (recvB[0:64] + recvB[64:128]).reshape(64, 128)
    rms = lax.rsqrt(heads[:, 96:97] / 2048.0 + EPS)
    heads = (heads * rms).astype(BF16).astype(F32)
    placed = jnp.where(here, dot(heads.astype(BF16), spread), 0.0).astype(BF16)
    maps = dot(group, placed)
    readout = silu(cio[0] + cio[1] * maps[:, 0:128]).astype(BF16)
    conv_input = silu(cio[2] + cio[3] * maps[:, 128:256])
    readout_f = readout.astype(F32)
    own_score = jnp.sum(readout_f * conv_input, axis=1, keepdims=True)
    own_row = jnp.sum(jnp.where(diag, own_score, 0.0), axis=0, keepdims=True)
    of_group = iota((64, 128), 0) >> 3
    blocks = jnp.concatenate(
        [jnp.where(of_group == g, readout_f, 0.0) for g in range(8)], axis=1
    ).astype(BF16)
    score = dot_t(blocks, v["binput"][...])
    weight = (faded * score).astype(BF16)
    from_block = diagonal(dot_t(v["binner"][...], weight), own_head)
    twice = jnp.concatenate([readout, readout], axis=1)
    from_state = diagonal(dot_t(s2[...], twice), own_head)
    by_channel = heads.T
    conv_inner = silu(cpi[...] + v["tinner"][3] * by_channel[32:64])
    mix = from_block + e_total * from_state + (own_row * step + v["skip"][...]) * conv_inner
    raw = mix * silu(by_channel[0:32])
    by_head = jnp.concatenate([raw, jnp.zeros((96, 64), F32)], axis=0).T
    packed = by_head[0:16]
    for q in range(1, 4):
        packed = packed + pltpu.roll(by_head[q * 16 : (q + 1) * 16], 32 * q, 1)
    srcC[...] = packed.astype(BF16)
    recvC[here_b] = packed.astype(BF16)
    to_last(2, lambda t: srcC, recvC)

    hid_swap.wait()
    for c in swaps[2:]:
        c.wait_recv()

    def unpacked(x):
        return jnp.concatenate([x[:, 0:64], x[:, 64:128]], axis=0)

    @pl.when(tp == 0)
    def _():
        pltpu.make_async_copy(pairF, pairF, pr.at[4]).wait()
        out_ref[...] = unpacked(pairF[...])

    @pl.when(tp == 1)
    def _():
        count(rs.at[3], recvW, 127)
        tiles = recvW[...].astype(F32).reshape(8, 128, 128)
        block = iota((128, 128), 1) >> 5
        for t in range(2):
            for dd in range(4):
                out = jnp.zeros((128, 128), F32)
                for q in range(4):
                    turned = tiles[t * 4 + q]
                    if q != dd:
                        turned = pltpu.roll(turned, (32 * (q - dd)) % 128, 1)
                    out = jnp.where(block == q, turned, out)
                out = out.astype(BF16).reshape(16, 8, 128)
                for i in range(16):
                    lanes = slice((i % 2) * 128, (i % 2) * 128 + 128)
                    wd[t * 8 + i // 2, dd * 8 : dd * 8 + 8, lanes] = out[i]
        count(rs.at[2], recvC, 127)
        gates = recvC[...].astype(F32)
        gf[...] = gates.reshape(2048, 128)
        partial = jnp.zeros((32, 64), F32)
        for t in range(2):
            for i in range(8):
                pair = [gf[pl.ds(t * 1024 + 2 * i + e, 64, stride=16), :] for e in range(2)]
                pair = jnp.concatenate(pair, axis=1).astype(BF16)
                partial = partial + dot_t(wd[t * 8 + i], pair)
        squares = jnp.sum(jnp.sum(gates * gates, axis=1), axis=1, keepdims=True)
        squares = squares[0:64] + squares[64:128]
        squares = jnp.sum(jnp.where(diag, squares, 0.0), axis=0, keepdims=True)
        squares = jnp.concatenate([squares, squares], axis=1)
        part0, part1 = halves(partial[0:16]), halves(partial[16:32])
        scale = lax.rsqrt(squares / 4096.0 + EPS)
        mids = []
        for t, (x, part) in enumerate(((otherA[...].astype(F32), part0), (x_own, part1))):
            mids.append((x + part * scale).astype(BF16))
            srcE[t] = mids[t]
            bufE[me, t] = mids[t]
        send_all(4, lambda t: srcE, bufE)
        for c in mine[2:]:
            c.wait()
        gain2 = v["cg"][...]
        we[...] = jnp.zeros((192, 2048), BF16)
        rpt[...] = jnp.zeros((128, 2048), F32)
        for t in range(2):
            we[t * 48 : t * 48 + 44] = (egF[t].astype(F32) * gain2).astype(BF16)
            we[96 + t * 48 : 96 + t * 48 + 44] = (evF[t].astype(F32) * gain2).astype(BF16)
            rpt[t * 48 : t * 48 + 44] = rpF[t].astype(F32)
        by_row = rpt[...].T.reshape(64, 4, 8, 128)
        for t in range(2):
            pick(we, we2.at[t], picked_of(t))
            for b in range(2):
                part = by_row[:, 2 * t + b].reshape(512, 128)
                rt[t, :, b * 128 : (b + 1) * 128] = part.astype(BF16)
        all_of(rs.at[4], bufE)
        y = bufE[...].astype(F32)
        squares2 = jnp.sum(jnp.sum(y * y, axis=(0, 1)), axis=0, keepdims=True)
        squares2 = squares2 + pltpu.roll(squares2, 64, 1)
        u = dot(we2[0], y[:, 0].reshape(512, 128).astype(BF16))
        u = u + dot(we2[1], y[:, 1].reshape(512, 128).astype(BF16))
        u = jnp.where(
            low_lanes,
            u[0:96] + pltpu.roll(u[192:288], 64, 1),
            pltpu.roll(u[96:192], 64, 1) + u[288:384],
        )
        u = u * lax.rsqrt(squares2 / 2048.0 + EPS)
        turned = pltpu.roll(u, 64, 1)
        act = silu(jnp.where(low_lanes, u, turned)) * jnp.where(low_lanes, turned, u)
        pad = jnp.zeros((32, 128), F32)
        aa = jnp.concatenate(
            [jnp.where(low_lanes, act, 0.0), pad, jnp.where(low_lanes, 0.0, act), pad], axis=0
        ).astype(BF16)
        for t in range(2):
            msgF[:, t] = dot(rt[t], aa).astype(BF16).reshape(64, 8, 128)
        recvF[me] = msgF[me]
        send_all(5, lambda t: msgF.at[t], recvF)
        all_of(rs.at[5], recvF)
        tot = jnp.sum(recvF[...].astype(F32), axis=0)
        sumF[...] = mids[0].astype(F32) + tot[0]
        c = swap(4, sumF, pairF)
        c.start()
        out_ref[...] = unpacked(mids[1].astype(F32) + tot[1])
        c.wait_send()
        all_of(ss.at[4], bufE)
        all_of(ss.at[5], recvF)

    @pl.when(tp == 0)
    def _():
        for c in mine[2:]:
            c.wait()
        count(ss.at[2], recvC, 64)
        count(ss.at[3], recvW, 64)

    for c in swaps[2:]:
        c.wait_send()

    @pl.when(tp == 1)
    def _():
        count(ss.at[2], recvC, 63)
        count(ss.at[3], recvW, 63)

    all_of(ss.at[0], bufA)
    pltpu.make_async_copy(parts, parts, ss.at[1]).wait()


def shards(
    hidden, mixer_gain, gate_proj, inner_proj, input_proj, output_proj, step_proj, step_bias,
    decay_log, skip_gain, taps_inner, taps_input, taps_output, recent_inner, recent_input,
    recent_output, states, block_inner, block_input, block_decay, lengths, norm_gain, mixer_out,
    channel_gain, expand_gate, expand_value, reduce_proj,
):
    args = dict(
        hid=hidden,
        mg=mixer_gain.reshape(1, 2048),
        gate=gate_proj.transpose(1, 2, 0).reshape(32, 2048),
        inner=inner_proj.transpose(1, 2, 0).reshape(32, 2048),
        inp=input_proj.T,
        outp=output_proj.T,
        stepw=step_proj.T,
        bias=step_bias.reshape(1, 64),
        dlog=decay_log.reshape(1, 64),
        skip=skip_gain.reshape(1, 64),
        tinner=taps_inner.transpose(0, 2, 1),
        tin=taps_input,
        tout=taps_output,
        rinner=recent_inner.transpose(0, 1, 3, 2).reshape(3, 32, 64),
        rin=recent_input.reshape(3, 1024),
        rout=recent_output.reshape(3, 1024),
        states=states.reshape(2048, 128),
        binner=block_inner.transpose(0, 2, 3, 1).reshape(2048, 128),
        binput=block_input.reshape(128, 1024),
        bdecay=block_decay.transpose(0, 2, 1).reshape(64, 128),
        lens=lengths.reshape(1, 1),
        normg=norm_gain.T,
        mo=mixer_out.reshape(32, 2048),
        cg=channel_gain.reshape(1, 2048),
        eg=expand_gate.T,
        ev=expand_value.T,
        rp=reduce_proj,
    )
    away = ("gate", "inner", "eg", "ev", "rp")
    near = [
        pltpu.VMEM(a.shape, a.dtype)
        for n, a in args.items()
        if n not in away
    ]
    scratch = near + [
        pltpu.VMEM((224, 2048), BF16),
        pltpu.VMEM((448, 512), BF16),
        pltpu.VMEM((2, 64, 2048), BF16),
        pltpu.VMEM((2, 44, 2048), BF16),
        pltpu.VMEM((2, 44, 2048), BF16),
        pltpu.VMEM((2, 44, 2048), BF16),
        pltpu.VMEM((192, 2048), BF16),
        pltpu.VMEM((2, 384, 512), BF16),
        pltpu.VMEM((16, 32, 256), BF16),
        pltpu.VMEM((2, 512, 256), BF16),
        pltpu.VMEM((128, 2048), F32),
        pltpu.VMEM((4, 64, 128), F32),
        pltpu.VMEM((32, 64), F32),
        pltpu.VMEM((64, 128), F32),
        pltpu.VMEM((2048, 256), BF16),
        pltpu.VMEM((2048, 128), F32),
        pltpu.VMEM((8, 128), BF16),
        pltpu.VMEM((N, 8, 128), BF16),
        pltpu.VMEM((2 * N, 1, 128), F32),
        pltpu.VMEM((2 * N, 1, 128), F32),
        pltpu.VMEM((8, 128), F32),
        pltpu.VMEM((8, 128), F32),
        pltpu.VMEM((8, 128), BF16),
        pltpu.VMEM((8, 128), F32),
        pltpu.VMEM((8, 128), F32),
        pltpu.VMEM((16, 128), BF16),
        pltpu.VMEM((2 * N, 16, 128), BF16),
        pltpu.VMEM((N, 8, 128), BF16),
        pltpu.VMEM((2 * N, 8, 128), BF16),
        pltpu.VMEM((2, 8, 128), BF16),
        pltpu.VMEM((N, 2, 8, 128), BF16),
        pltpu.VMEM((N, 2, 8, 128), BF16),
        pltpu.VMEM((N, 2, 8, 128), BF16),
        pltpu.SemaphoreType.DMA((len(near),)),
        pltpu.SemaphoreType.DMA((5,)),
        pltpu.SemaphoreType.DMA((5,)),
        pltpu.SemaphoreType.DMA((5,)),
        pltpu.SemaphoreType.DMA((6,)),
        pltpu.SemaphoreType.DMA((6,)),
        pltpu.SemaphoreType.DMA((6,)),
        pltpu.SemaphoreType.DMA((6,)),
    ]
    space = [
        pl.BlockSpec(memory_space=pltpu.HBM if n == "lens" else pl.ANY) for n in args
    ]
    end = pl.pallas_call(
        kernel,
        out_shape=pltpu.VMEM((16, 64), F32),
        in_specs=space,
        out_specs=pl.BlockSpec(memory_space=pltpu.VMEM),
        scratch_shapes=scratch,
        compiler_params=pltpu.CompilerParams(collective_id=0, has_side_effects=True),
    )(*args.values())
    return end.astype(BF16)


def solution(mesh):
    in_specs = (
        P(KV_TP, "dp"),
        P(),
        P(None, "kv", "tp"),
        P(None, "kv", "tp"),
        P(None, "kv"),
        P(None, "kv"),
        P(),
        P(),
        P(),
        P(),
        P(None, None, "tp"),
        P(),
        P(),
        P(DP_KV, None, None, "tp"),
        P(DP_KV, None, None),
        P(DP_KV, None, None),
        P(DP_KV, None, "tp", None),
        P(DP_KV, None, None, "tp"),
        P(DP_KV, None, None),
        P(DP_KV, None, None),
        P(DP_KV),
        P(None, "tp"),
        P("kv", "tp", None),
        P(),
        P(None, KV_TP),
        P(None, KV_TP),
        P(KV_TP, None),
    )
    return jax.shard_map(
        shards, mesh=mesh, in_specs=in_specs, out_specs=P(KV_TP, "dp"), check_vma=False
    )
```

```python
import jax
import jax.numpy as jnp
from jax import lax
from jax.experimental import pallas as pl
from jax.experimental.pallas import tpu as pltpu
from jax.sharding import PartitionSpec as P

F32 = jnp.float32
BF16 = jnp.bfloat16
MESH = pl.DeviceIdType.MESH
EPS = 1e-05
N = 64
DP_KV = ("dp", "kv")
KV_TP = ("kv", "tp")
NAMES = (
    "hid",
    "mg",
    "gate",
    "inner",
    "inp",
    "outp",
    "stepw",
    "bias",
    "dlog",
    "skip",
    "tinner",
    "tin",
    "tout",
    "rinner",
    "rin",
    "rout",
    "states",
    "binner",
    "binput",
    "bdecay",
    "lens",
    "normg",
    "mo",
    "cg",
    "eg",
    "ev",
    "rp",
)


def silu(v):
    return v / (1.0 + jnp.exp(-v))


def iota(shape, dim):
    return lax.broadcasted_iota(jnp.int32, shape, dim)


def dot(a, b):
    return jnp.dot(a, b, preferred_element_type=F32)


def dot_t(a, b):
    return lax.dot_general(a, b, (((1,), (1,)), ((), ())), preferred_element_type=F32)


def halves(x):
    return jnp.concatenate([x[:8, :], x[8:, :]], axis=1)


def diagonal(d, mask):
    return jnp.sum(jnp.where(mask, d.reshape(64, 32, 64), 0.0), axis=0)


def kernel(*refs):
    names = NAMES
    h = dict(zip(names, refs))
    out_ref = refs[len(names)]
    local = [n for n in names if n not in ("gate", "inner", "eg", "ev", "rp")]
    rest = refs[len(names) + 1 :]
    v = dict(zip(local, rest))
    (
        wfull, wproj, giF, egF, evF, rpF, we, we2, wd, rt, rpt, cio, cpi, msuf, s2, gf,
        srcA, bufA, msgB, recvB, sumA, pairA, otherA, sumF, pairF, srcC, recvC, msgW, recvW, srcE, bufE, msgF, recvF,
        lsem, csem, xs, xr, ss, rs, ps, pr,
    ) = rest[len(local) :]
    me, tp = lax.axis_index("kv"), lax.axis_index("tp")
    here_b = tp * N + me

    order = (4, 3, 5, 2, 6, 1, 7, 0)
    in_rows = [lax.rem(me // 8 + o, 8) * 8 for o in order]
    in_cols = [lax.rem(lax.rem(me, 8) + o, 8) for o in order]
    peers = [r + c for r in in_rows for c in in_cols][: N - 1]
    dist = [min(o, 8 - o) for o in order]
    ranks = sorted(range(N - 1), key=lambda i: -(dist[i // 8] + dist[i % 8]))
    peers = [peers[i] for i in ranks]

    barrier = pltpu.get_barrier_semaphore()

    pl.semaphore_signal(barrier, inc=1, device_id={"tp": 1 - tp}, device_id_type=MESH)
    for t in peers:
        pl.semaphore_signal(barrier, inc=1, device_id={"kv": t}, device_id_type=MESH)

    loads = {n: pltpu.make_async_copy(h[n], v[n], lsem.at[i]) for i, n in enumerate(local)}
    shared = (
        ("gate", giF.at[tp, pl.ds(0, 32)]),
        ("inner", giF.at[tp, pl.ds(32, 32)]),
        ("eg", egF.at[tp]),
        ("ev", evF.at[tp]),
        ("rp", rpF.at[tp]),
    )
    mine = [pltpu.make_async_copy(h[n], f, csem.at[i]) for i, (n, f) in enumerate(shared)]
    for c in loads.values():
        c.start()
    for c in mine:
        c.start()

    def send_all(p, source, target):
        def one(i, c):
            t = i
            pltpu.make_async_remote_copy(
                src_ref=source(t),
                dst_ref=target.at[me],
                send_sem=ss.at[p],
                recv_sem=rs.at[p],
                device_id={"kv": t},
                device_id_type=MESH,
            ).start()
            return c

        for t in peers:
            one(t, 0)

    def to_last(p, source, target):
        def one(t):
            pltpu.make_async_remote_copy(
                src_ref=source(me if t is None else t),
                dst_ref=target.at[here_b],
                send_sem=ss.at[p],
                recv_sem=rs.at[p],
                device_id={"tp": 1} if t is None else {"kv": t, "tp": 1},
                device_id_type=MESH,
            ).start()

        for t in peers:
            one(t)

        @pl.when(tp == 0)
        def _():
            one(None)

    def count(sem, buf, n):
        some = buf.at[pl.ds(0, n)]
        pltpu.make_async_copy(some, some, sem).wait()

    def all_of(sem, buf):
        most = buf.at[pl.ds(0, N - 1)]
        pltpu.make_async_copy(most, most, sem).wait()

    def swap(p, source, target):
        return pltpu.make_async_remote_copy(
            src_ref=source,
            dst_ref=target,
            send_sem=ps.at[p],
            recv_sem=pr.at[p],
            device_id={"tp": 1 - tp},
            device_id_type=MESH,
        )

    loads["hid"].wait()
    x_own = halves(v["hid"][...].astype(F32))
    srcA[...] = x_own.astype(BF16)
    bufA[me] = x_own.astype(BF16)
    pl.semaphore_wait(barrier, N)

    send_all(0, lambda t: srcA, bufA)
    hid_swap = swap(5, srcA, otherA)
    hid_swap.start()
    swaps = [
        pltpu.make_async_remote_copy(
            src_ref=h[n],
            dst_ref=f,
            send_sem=xs.at[i],
            recv_sem=xr.at[i],
            device_id={"tp": 1 - tp},
            device_id_type=MESH,
        )
        for i, (n, f) in enumerate(shared)
    ]
    for c in swaps:
        c.start()
    for n in local:
        if n != "hid":
            loads[n].wait()

    gain = v["mg"][...]
    wfull[128:144] = (v["inp"][...].astype(F32) * gain).astype(BF16)
    wfull[144:160] = (v["outp"][...].astype(F32) * gain).astype(BF16)
    wfull[160:224] = (v["stepw"][...].astype(F32) * gain).astype(BF16)
    low_lanes = iota((1, 128), 1) < 64
    to, at = iota((512, 256), 0), iota((512, 256), 1)
    spot = ((at & 127) >> 3) * 32 + (at >> 7) * 8 + (at & 7)

    def picked_of(t):
        return (to == spot + 16 * t).astype(BF16)

    def pick(whole, out, picked):
        n = whole.shape[0]
        for i in range(4):
            y = dot(whole[:, i * 512 : (i + 1) * 512], picked).astype(BF16)
            out[0:n, i * 128 : (i + 1) * 128] = y[:, 0:128]
            out[n : 2 * n, i * 128 : (i + 1) * 128] = y[:, 128:256]

    for c in mine[:2]:
        c.wait()
    for c in swaps[:2]:
        c.wait()
    for t in range(2):
        wfull[t * 64 : t * 64 + 64] = (giF[t].astype(F32) * gain).astype(BF16)
    pick(wfull, wproj, picked_of(tp))

    for a, (t, r) in enumerate((("tout", "rout"), ("tin", "rin"))):
        taps, rec = v[t][...], v[r][...].astype(F32)
        past = jnp.sum(rec * taps[:3], axis=0, keepdims=True)
        for g in range(8):
            at = slice(g * 128, (g + 1) * 128)
            cio[2 * a, g * 8 : (g + 1) * 8] = jnp.broadcast_to(past[:, at], (8, 128))
            cio[2 * a + 1, g * 8 : (g + 1) * 8] = jnp.broadcast_to(taps[3:4, at], (8, 128))
    taps, rec = v["tinner"], v["rinner"]
    cpi[...] = (
        taps[0] * rec[0].astype(F32) + taps[1] * rec[1].astype(F32) + taps[2] * rec[2].astype(F32)
    )

    live = (iota((64, 128), 1) < v["lens"][0:1, 0:1]).astype(F32)
    masked = v["bdecay"][...] * live
    later = (iota((128, 128), 0) > iota((128, 128), 1)).astype(F32)
    msuf[...] = jnp.dot(
        masked, later, preferred_element_type=F32, precision=lax.Precision.HIGHEST
    )
    diag = iota((64, 64), 0) == iota((64, 64), 1)
    cached = jnp.sum(masked, axis=1, keepdims=True)
    cached_row = jnp.sum(jnp.where(diag, cached, 0.0), axis=0, keepdims=True)
    whole = v["states"][...]
    high = whole.astype(BF16)
    s2[:, 0:128] = high
    s2[:, 128:256] = (whole - high.astype(F32)).astype(BF16)

    lane = iota((32, 64), 1)
    norm = jnp.sum(jnp.where(lane == me, v["normg"][...], 0.0), axis=1, keepdims=True)
    rows = jnp.concatenate([v["mo"][...].astype(F32) * norm, jnp.zeros((96, 2048), F32)], axis=0)
    rows = rows.T.reshape(64, 4, 8, 128)
    packed = rows[:, 0].reshape(512, 128)
    for q in range(1, 4):
        packed = packed + pltpu.roll(rows[:, q].reshape(512, 128), 32 * q, 1)
    msgW[...] = packed.astype(BF16).reshape(64, 8, 128)
    recvW[here_b] = msgW[me]

    def gathered(p, buf, w):
        all_of(rs.at[p], buf)
        x = buf[...].astype(F32)
        squares = jnp.sum(jnp.sum(x * x, axis=0), axis=0, keepdims=True)
        squares = squares + pltpu.roll(squares, 64, 1)
        return dot(w[...], x.reshape(512, 128).astype(BF16)), squares

    u, squares = gathered(0, bufA, wproj)
    u = u[0:224] + pltpu.roll(u[224:448], 64, 1)
    tail = jnp.concatenate(
        [u[128:160], jnp.broadcast_to(squares, (8, 128)), jnp.zeros((24, 128), F32)], axis=0
    )
    by_core = [jnp.concatenate([u[t * 64 : t * 64 + 64], tail], axis=0) for t in range(2)]
    by_seq = jnp.where(low_lanes, by_core[0], pltpu.roll(by_core[1], 64, 1)).T
    msgB[...] = by_seq.reshape(128, 1, 128)
    recvB[here_b] = msgB[here_b]

    def send_parts(i, c):
        t = i
        for core in range(2):
            pltpu.make_async_remote_copy(
                src_ref=msgB.at[core * N + t],
                dst_ref=recvB.at[here_b],
                send_sem=ss.at[1],
                recv_sem=rs.at[1],
                device_id={"kv": t, "tp": core},
                device_id_type=MESH,
            ).start()
        return c

    for t in peers:
        send_parts(t, 0)
    pltpu.make_async_remote_copy(
        src_ref=msgB.at[(1 - tp) * N + me],
        dst_ref=recvB.at[here_b],
        send_sem=ss.at[1],
        recv_sem=rs.at[1],
        device_id={"tp": 1 - tp},
        device_id_type=MESH,
    ).start()
    step_col = jnp.sum(
        jnp.where(iota((64, 128), 1) == me, u[160:224], 0.0), axis=1, keepdims=True
    )
    step_row = jnp.sum(jnp.where(diag, step_col, 0.0), axis=0, keepdims=True)
    sumA[0:1, 0:64] = step_row
    sumA[1:2, :] = squares
    own_swap = swap(0, sumA, pairA)
    own_swap.start()
    own_swap.wait()
    squares = jnp.where(iota((1, 128), 1) == me, squares + pairA[1:2], 0.0)
    own_rms = lax.rsqrt(jnp.sum(squares, axis=1, keepdims=True) / 2048.0 + EPS)
    step_pre = (own_rms * (step_row + pairA[0:1, 0:64])).astype(BF16).astype(F32)
    shifted = step_pre + v["bias"][...]
    step = jnp.maximum(shifted, 0.0) + jnp.log1p(jnp.exp(-jnp.abs(shifted)))
    decay = -jnp.exp(v["dlog"][...]) * step
    e_total = jnp.exp(decay + cached_row)
    decay_col = jnp.sum(jnp.where(diag, decay, 0.0), axis=1, keepdims=True)
    faded = live * jnp.exp(decay_col + msuf[...])

    n_of, k_of = iota((128, 256), 1), iota((128, 256), 0)
    base = jnp.where(n_of < 128, 80, 64)
    spread = ((k_of - base) == (n_of & 15)).astype(BF16)
    here = ((iota((64, 256), 1) & 127) >> 4) == (iota((64, 256), 0) & 7)
    group = ((iota((64, 64), 0) >> 3) == (iota((64, 64), 1) >> 3)).astype(BF16)
    own_head = iota((64, 32, 64), 0) == iota((64, 32, 64), 2)
    to_last(3, lambda t: msgW.at[t], recvW)

    parts = recvB.at[pl.ds(0, 127)]
    pltpu.make_async_copy(parts, parts, rs.at[1]).wait()
    heads = (recvB[0:64] + recvB[64:128]).reshape(64, 128)
    rms = lax.rsqrt(heads[:, 96:97] / 2048.0 + EPS)
    heads = (heads * rms).astype(BF16).astype(F32)
    placed = jnp.where(here, dot(heads.astype(BF16), spread), 0.0).astype(BF16)
    maps = dot(group, placed)
    readout = silu(cio[0] + cio[1] * maps[:, 0:128]).astype(BF16)
    conv_input = silu(cio[2] + cio[3] * maps[:, 128:256])
    readout_f = readout.astype(F32)
    own_score = jnp.sum(readout_f * conv_input, axis=1, keepdims=True)
    own_row = jnp.sum(jnp.where(diag, own_score, 0.0), axis=0, keepdims=True)
    of_group = iota((64, 128), 0) >> 3
    blocks = jnp.concatenate(
        [jnp.where(of_group == g, readout_f, 0.0) for g in range(8)], axis=1
    ).astype(BF16)
    score = dot_t(blocks, v["binput"][...])
    weight = (faded * score).astype(BF16)
    from_block = diagonal(dot_t(v["binner"][...], weight), own_head)
    twice = jnp.concatenate([readout, readout], axis=1)
    from_state = diagonal(dot_t(s2[...], twice), own_head)
    by_channel = heads.T
    conv_inner = silu(cpi[...] + v["tinner"][3] * by_channel[32:64])
    mix = from_block + e_total * from_state + (own_row * step + v["skip"][...]) * conv_inner
    raw = mix * silu(by_channel[0:32])
    by_head = jnp.concatenate([raw, jnp.zeros((96, 64), F32)], axis=0).T
    packed = by_head[0:16]
    for q in range(1, 4):
        packed = packed + pltpu.roll(by_head[q * 16 : (q + 1) * 16], 32 * q, 1)
    srcC[...] = packed.astype(BF16)
    recvC[here_b] = packed.astype(BF16)
    to_last(2, lambda t: srcC, recvC)

    hid_swap.wait()
    for c in swaps[2:]:
        c.wait_recv()

    def unpacked(x):
        return jnp.concatenate([x[:, 0:64], x[:, 64:128]], axis=0)

    @pl.when(tp == 0)
    def _():
        pltpu.make_async_copy(pairF, pairF, pr.at[4]).wait()
        out_ref[...] = unpacked(pairF[...])

    @pl.when(tp == 1)
    def _():
        count(rs.at[3], recvW, 127)
        tiles = recvW[...].astype(F32).reshape(8, 128, 128)
        block = iota((128, 128), 1) >> 5
        for t in range(2):
            for dd in range(4):
                out = jnp.zeros((128, 128), F32)
                for q in range(4):
                    turned = tiles[t * 4 + q]
                    if q != dd:
                        turned = pltpu.roll(turned, (32 * (q - dd)) % 128, 1)
                    out = jnp.where(block == q, turned, out)
                out = out.astype(BF16).reshape(16, 8, 128)
                for i in range(16):
                    lanes = slice((i % 2) * 128, (i % 2) * 128 + 128)
                    wd[t * 8 + i // 2, dd * 8 : dd * 8 + 8, lanes] = out[i]
        count(rs.at[2], recvC, 127)
        gates = recvC[...].astype(F32)
        gf[...] = gates.reshape(2048, 128)
        partial = jnp.zeros((32, 64), F32)
        for t in range(2):
            for i in range(8):
                pair = [gf[pl.ds(t * 1024 + 2 * i + e, 64, stride=16), :] for e in range(2)]
                pair = jnp.concatenate(pair, axis=1).astype(BF16)
                partial = partial + dot_t(wd[t * 8 + i], pair)
        squares = jnp.sum(jnp.sum(gates * gates, axis=1), axis=1, keepdims=True)
        squares = squares[0:64] + squares[64:128]
        squares = jnp.sum(jnp.where(diag, squares, 0.0), axis=0, keepdims=True)
        squares = jnp.concatenate([squares, squares], axis=1)
        part0, part1 = halves(partial[0:16]), halves(partial[16:32])
        scale = lax.rsqrt(squares / 4096.0 + EPS)
        mids = []
        for t, (x, part) in enumerate(((otherA[...].astype(F32), part0), (x_own, part1))):
            mids.append((x + part * scale).astype(BF16))
            srcE[t] = mids[t]
            bufE[me, t] = mids[t]
        send_all(4, lambda t: srcE, bufE)
        for c in mine[2:]:
            c.wait()
        gain2 = v["cg"][...]
        we[...] = jnp.zeros((192, 2048), BF16)
        rpt[...] = jnp.zeros((128, 2048), F32)
        for t in range(2):
            we[t * 48 : t * 48 + 44] = (egF[t].astype(F32) * gain2).astype(BF16)
            we[96 + t * 48 : 96 + t * 48 + 44] = (evF[t].astype(F32) * gain2).astype(BF16)
            rpt[t * 48 : t * 48 + 44] = rpF[t].astype(F32)
        by_row = rpt[...].T.reshape(64, 4, 8, 128)
        for t in range(2):
            pick(we, we2.at[t], picked_of(t))
            for b in range(2):
                part = by_row[:, 2 * t + b].reshape(512, 128)
                rt[t, :, b * 128 : (b + 1) * 128] = part.astype(BF16)
        all_of(rs.at[4], bufE)
        y = bufE[...].astype(F32)
        squares2 = jnp.sum(jnp.sum(y * y, axis=(0, 1)), axis=0, keepdims=True)
        squares2 = squares2 + pltpu.roll(squares2, 64, 1)
        u = dot(we2[0], y[:, 0].reshape(512, 128).astype(BF16))
        u = u + dot(we2[1], y[:, 1].reshape(512, 128).astype(BF16))
        u = jnp.where(
            low_lanes,
            u[0:96] + pltpu.roll(u[192:288], 64, 1),
            pltpu.roll(u[96:192], 64, 1) + u[288:384],
        )
        u = u * lax.rsqrt(squares2 / 2048.0 + EPS)
        turned = pltpu.roll(u, 64, 1)
        act = silu(jnp.where(low_lanes, u, turned)) * jnp.where(low_lanes, turned, u)
        pad = jnp.zeros((32, 128), F32)
        aa = jnp.concatenate(
            [jnp.where(low_lanes, act, 0.0), pad, jnp.where(low_lanes, 0.0, act), pad], axis=0
        ).astype(BF16)
        for t in range(2):
            msgF[:, t] = dot(rt[t], aa).astype(BF16).reshape(64, 8, 128)
        recvF[me] = msgF[me]
        send_all(5, lambda t: msgF.at[t], recvF)
        all_of(rs.at[5], recvF)
        sumF[...] = mids[0].astype(F32) + jnp.sum(recvF[:, 0].astype(F32), axis=0)
        c = swap(4, sumF, pairF)
        c.start()
        out_ref[...] = unpacked(mids[1].astype(F32) + jnp.sum(recvF[:, 1].astype(F32), axis=0))
        c.wait_send()
        all_of(ss.at[4], bufE)
        all_of(ss.at[5], recvF)

    @pl.when(tp == 0)
    def _():
        for c in mine[2:]:
            c.wait()
        count(ss.at[2], recvC, 64)
        count(ss.at[3], recvW, 64)

    for c in swaps[2:]:
        c.wait_send()

    @pl.when(tp == 1)
    def _():
        count(ss.at[2], recvC, 63)
        count(ss.at[3], recvW, 63)

    all_of(ss.at[0], bufA)
    pltpu.make_async_copy(parts, parts, ss.at[1]).wait()


def shards(
    hidden, mixer_gain, gate_proj, inner_proj, input_proj, output_proj, step_proj, step_bias,
    decay_log, skip_gain, taps_inner, taps_input, taps_output, recent_inner, recent_input,
    recent_output, states, block_inner, block_input, block_decay, lengths, norm_gain, mixer_out,
    channel_gain, expand_gate, expand_value, reduce_proj,
):
    args = dict(
        hid=hidden,
        mg=mixer_gain.reshape(1, 2048),
        gate=gate_proj.transpose(1, 2, 0).reshape(32, 2048),
        inner=inner_proj.transpose(1, 2, 0).reshape(32, 2048),
        inp=input_proj.T,
        outp=output_proj.T,
        stepw=step_proj.T,
        bias=step_bias.reshape(1, 64),
        dlog=decay_log.reshape(1, 64),
        skip=skip_gain.reshape(1, 64),
        tinner=taps_inner.transpose(0, 2, 1),
        tin=taps_input,
        tout=taps_output,
        rinner=recent_inner.transpose(0, 1, 3, 2).reshape(3, 32, 64),
        rin=recent_input.reshape(3, 1024),
        rout=recent_output.reshape(3, 1024),
        states=states.reshape(2048, 128),
        binner=block_inner.transpose(0, 2, 3, 1).reshape(2048, 128),
        binput=block_input.reshape(128, 1024),
        bdecay=block_decay.transpose(0, 2, 1).reshape(64, 128),
        lens=lengths.reshape(1, 1),
        normg=norm_gain.T,
        mo=mixer_out.reshape(32, 2048),
        cg=channel_gain.reshape(1, 2048),
        eg=expand_gate.T,
        ev=expand_value.T,
        rp=reduce_proj,
    )
    away = ("gate", "inner", "eg", "ev", "rp")
    near = [
        pltpu.VMEM(a.shape, a.dtype)
        for n, a in args.items()
        if n not in away
    ]
    scratch = near + [
        pltpu.VMEM((224, 2048), BF16),
        pltpu.VMEM((448, 512), BF16),
        pltpu.VMEM((2, 64, 2048), BF16),
        pltpu.VMEM((2, 44, 2048), BF16),
        pltpu.VMEM((2, 44, 2048), BF16),
        pltpu.VMEM((2, 44, 2048), BF16),
        pltpu.VMEM((192, 2048), BF16),
        pltpu.VMEM((2, 384, 512), BF16),
        pltpu.VMEM((16, 32, 256), BF16),
        pltpu.VMEM((2, 512, 256), BF16),
        pltpu.VMEM((128, 2048), F32),
        pltpu.VMEM((4, 64, 128), F32),
        pltpu.VMEM((32, 64), F32),
        pltpu.VMEM((64, 128), F32),
        pltpu.VMEM((2048, 256), BF16),
        pltpu.VMEM((2048, 128), F32),
        pltpu.VMEM((8, 128), BF16),
        pltpu.VMEM((N, 8, 128), BF16),
        pltpu.VMEM((2 * N, 1, 128), F32),
        pltpu.VMEM((2 * N, 1, 128), F32),
        pltpu.VMEM((8, 128), F32),
        pltpu.VMEM((8, 128), F32),
        pltpu.VMEM((8, 128), BF16),
        pltpu.VMEM((8, 128), F32),
        pltpu.VMEM((8, 128), F32),
        pltpu.VMEM((16, 128), BF16),
        pltpu.VMEM((2 * N, 16, 128), BF16),
        pltpu.VMEM((N, 8, 128), BF16),
        pltpu.VMEM((2 * N, 8, 128), BF16),
        pltpu.VMEM((2, 8, 128), BF16),
        pltpu.VMEM((N, 2, 8, 128), BF16),
        pltpu.VMEM((N, 2, 8, 128), BF16),
        pltpu.VMEM((N, 2, 8, 128), BF16),
        pltpu.SemaphoreType.DMA((len(near),)),
        pltpu.SemaphoreType.DMA((5,)),
        pltpu.SemaphoreType.DMA((5,)),
        pltpu.SemaphoreType.DMA((5,)),
        pltpu.SemaphoreType.DMA((6,)),
        pltpu.SemaphoreType.DMA((6,)),
        pltpu.SemaphoreType.DMA((6,)),
        pltpu.SemaphoreType.DMA((6,)),
    ]
    space = [
        pl.BlockSpec(memory_space=pltpu.HBM if n == "lens" else pl.ANY) for n in args
    ]
    end = pl.pallas_call(
        kernel,
        out_shape=pltpu.VMEM((16, 64), F32),
        in_specs=space,
        out_specs=pl.BlockSpec(memory_space=pltpu.VMEM),
        scratch_shapes=scratch,
        compiler_params=pltpu.CompilerParams(collective_id=0, has_side_effects=True),
    )(*args.values())
    return end.astype(BF16)


def solution(mesh):
    in_specs = (
        P(KV_TP, "dp"),
        P(),
        P(None, "kv", "tp"),
        P(None, "kv", "tp"),
        P(None, "kv"),
        P(None, "kv"),
        P(),
        P(),
        P(),
        P(),
        P(None, None, "tp"),
        P(),
        P(),
        P(DP_KV, None, None, "tp"),
        P(DP_KV, None, None),
        P(DP_KV, None, None),
        P(DP_KV, None, "tp", None),
        P(DP_KV, None, None, "tp"),
        P(DP_KV, None, None),
        P(DP_KV, None, None),
        P(DP_KV),
        P(None, "tp"),
        P("kv", "tp", None),
        P(),
        P(None, KV_TP),
        P(None, KV_TP),
        P(KV_TP, None),
    )
    return jax.shard_map(
        shards, mesh=mesh, in_specs=in_specs, out_specs=P(KV_TP, "dp"), check_vma=False
    )
```
